32 devices in a mesh: grp: 2 (over y), sp: 4 (over z), tp: 4 (over x, core).
Axes of the slice: x: 2, y: 2, z: 4, core: 2. Of those that a mesh axis runs over, the one named last changes fastest.
Arguments:
- inputs: bfloat16 [2048, 2048], P(('grp', 'sp')), parts along dimension 0, may hold values from -6 to 6
- norm_gain: float32 [2048], replicated, may hold values from 0.1 to 1.9
- da_query_weight: bfloat16 [2048, 1024], P('sp', 'tp'), may hold values from -0.125 to 0.125
- da_key_weight: bfloat16 [2048, 1024], P('sp', 'tp'), may hold values from -0.125 to 0.125
- da_value_weight: bfloat16 [2048, 1024], P('sp', 'tp'), may hold values from -0.125 to 0.125
- sw_query_weight: bfloat16 [2048, 1024], P('sp', 'tp'), may hold values from -0.125 to 0.125
- sw_key_weight: bfloat16 [2048, 512], P('sp', 'tp'), may hold values from -0.125 to 0.125
- sw_value_weight: bfloat16 [2048, 512], P('sp', 'tp'), may hold values from -0.125 to 0.125
- da_query_gain: float32 [64], replicated, may hold values from 0.6 to 30
- da_key_gain: float32 [64], replicated, may hold values from 0.6 to 30
- sw_query_gain: float32 [64], replicated, may hold values from 0.6 to 30
- sw_key_gain: float32 [64], replicated, may hold values from 0.6 to 30
- mix_lambda: float32 [8], P('tp'), may hold values from 0.3 to 0.8
- head_gain: float32 [128], replicated, may hold values from 0.1 to 1.9
- sink_logit: float32 [16], P('tp'), may hold values from 0 to 8
- da_out_weight: bfloat16 [1024, 2048], P('tp'), may hold values from -0.1875 to 0.1875
- sw_out_weight: bfloat16 [1024, 2048], P('tp'), may hold values from -0.1875 to 0.1875
Outputs:
- mixed: bfloat16 [2048, 2048], P(('grp', 'sp')), parts along dimension 0
The draws below stay inside these ranges and needn't reach their ends.
There are 2 independent parts, one for each index of `grp`. The reference program is written for one: setup_inputs(seed, part) draws one part's arguments, and reference() takes and returns one part's arrays. A program takes and returns all parts, laid end to end along the dimension named above; an argument that names none is the same for every part. Nothing has to cross between parts.
All inputs are finite; a program needn't handle non-finite values.
Results may differ from the reference program's by a relative error of at most 0.014.
The reference program's roundings to bfloat16 on the way count: a program that leaves them out, or rounds other values in their place, can miss the bound.
Values may be sent and summed in bfloat16 or wider, within the bound.
A program may use at most 64 MiB of HBM per device.

```python
import math
import jax
import jax.numpy as jnp
from jax import lax

D = 2048
DA_HEADS = 8
SW_HEADS = 16
KV_HEADS = 8
HD = 64
WINDOW = 128
SEQ = 1024
N_TP = 4


def gain_draw(key, own):
    values = jax.random.uniform(jax.random.fold_in(key, own), (HD,), jnp.float32, 0.6, 2.4)
    return values


def draw_da_query_gain(key, part):
    return gain_draw(key, 11)


def draw_da_key_gain(key, part):
    return gain_draw(key, 12)


def draw_sw_query_gain(key, part):
    return gain_draw(key, 13)


def draw_sw_key_gain(key, part):
    return gain_draw(key, 14)


def level_of(key, extent, cuts, smallest, top_value):
    def one(dim, shards_of):
        steps = jax.random.uniform(jax.random.fold_in(jax.random.fold_in(key, 6), dim), (shards_of,), jnp.float32, smallest / len(cuts), top_value / len(cuts))
        return jnp.repeat(jnp.exp(steps), extent[dim] // shards_of).reshape((-1,) + (1,) * (len(extent) - dim - 1))

    loudness = one(*cuts[0])
    for cut in cuts[1:]:
        loudness = loudness * one(*cut)
    return loudness


def bell_draw(key, shape, width, reach, shards=(), held_as=jnp.bfloat16):
    entries = width * jax.random.normal(key, shape, jnp.float32)
    if shards:
        entries = entries * level_of(key, shape, shards, -0.22, 0.18)
    return jnp.clip(entries, -reach, reach).astype(held_as)


def setup_inputs(seed: int = 0, part: int = 0) -> dict:
    keys = jax.random.split(jax.random.key(seed), 18)
    own_keys = jax.random.split(jax.random.fold_in(keys[17], part), 18)
    inputs = bell_draw(own_keys[0], (SEQ, D), 1.0, 6.0, ((0, 4),))
    norm_gain = jnp.clip(1.0 + 0.18 * jax.random.normal(keys[1], (D,), jnp.float32), 0.1, 1.9)
    da_query_weight = bell_draw(keys[2], (D, DA_HEADS * 2 * HD), D ** -0.5, 0.125, ((0, 4), (1, 4)))
    da_key_weight = bell_draw(keys[3], (D, DA_HEADS * 2 * HD), D ** -0.5, 0.125, ((0, 4), (1, 4)))
    da_value_weight = bell_draw(keys[4], (D, DA_HEADS * 2 * HD), D ** -0.5, 0.125, ((0, 4), (1, 4)))
    sw_query_weight = bell_draw(keys[5], (D, SW_HEADS * HD), D ** -0.5, 0.125, ((0, 4), (1, 4)))
    sw_key_weight = bell_draw(keys[6], (D, KV_HEADS * HD), D ** -0.5, 0.125, ((0, 4), (1, 4)))
    sw_value_weight = bell_draw(keys[7], (D, KV_HEADS * HD), D ** -0.5, 0.125, ((0, 4), (1, 4)))
    da_query_gain = draw_da_query_gain(jax.random.fold_in(keys[17], 71), part)
    da_key_gain = draw_da_key_gain(jax.random.fold_in(keys[17], 71), part)
    sw_query_gain = draw_sw_query_gain(jax.random.fold_in(keys[17], 71), part)
    sw_key_gain = draw_sw_key_gain(jax.random.fold_in(keys[17], 71), part)
    mix_lambda = jnp.clip(0.3 + 0.5 * jax.random.uniform(keys[12], (DA_HEADS,), jnp.float32) ** level_of(keys[12], (DA_HEADS,), ((0, 4),), -0.2, 0.2), 0.3, 0.8)
    head_gain = jnp.clip(1.0 + 0.18 * jax.random.normal(keys[13], (2 * HD,), jnp.float32), 0.1, 1.9)
    sink_logit = jnp.clip(8.0 * jax.random.uniform(keys[14], (SW_HEADS,), jnp.float32) ** level_of(keys[14], (SW_HEADS,), ((0, 4),), -0.2, 0.2), 0.0, 8.0)
    da_out_weight = bell_draw(keys[15], (DA_HEADS * 2 * HD, D), (DA_HEADS * 2 * HD) ** -0.5, 0.1875, ((0, 4),))
    sw_out_weight = bell_draw(keys[16], (SW_HEADS * HD, D), (SW_HEADS * HD) ** -0.5, 0.1875, ((0, 4),))
    return {"inputs": inputs, "norm_gain": norm_gain, "da_query_weight": da_query_weight, "da_key_weight": da_key_weight, "da_value_weight": da_value_weight, "sw_query_weight": sw_query_weight, "sw_key_weight": sw_key_weight, "sw_value_weight": sw_value_weight, "da_query_gain": da_query_gain, "da_key_gain": da_key_gain, "sw_query_gain": sw_query_gain, "sw_key_gain": sw_key_gain, "mix_lambda": mix_lambda, "head_gain": head_gain, "sink_logit": sink_logit, "da_out_weight": da_out_weight, "sw_out_weight": sw_out_weight}


def rms_norm(values, gain):
    return values * lax.rsqrt(lax.optimization_barrier(jnp.mean(values * values, axis=-1, keepdims=True)) + 1e-06) * gain

def reference(inputs, norm_gain, da_query_weight, da_key_weight, da_value_weight, sw_query_weight, sw_key_weight, sw_value_weight, da_query_gain, da_key_gain, sw_query_gain, sw_key_gain, mix_lambda, head_gain, sink_logit, da_out_weight, sw_out_weight):
    length = inputs.shape[0]
    normed = rms_norm(inputs.astype(jnp.float32), norm_gain).astype(jnp.bfloat16)

    def project(matrix):
        return jnp.dot(normed, matrix, preferred_element_type=jnp.float32)
    da_query = rms_norm(project(da_query_weight).reshape(length, DA_HEADS, 2, HD), da_query_gain).astype(jnp.bfloat16)
    da_key = rms_norm(project(da_key_weight).reshape(length, DA_HEADS, 2, HD), da_key_gain).astype(jnp.bfloat16)
    da_value = project(da_value_weight).astype(jnp.bfloat16).reshape(length, DA_HEADS, 2 * HD)
    sw_query = rms_norm(project(sw_query_weight).reshape(length, SW_HEADS, HD), sw_query_gain).astype(jnp.bfloat16)
    sw_key = rms_norm(project(sw_key_weight).reshape(length, KV_HEADS, HD), sw_key_gain).astype(jnp.bfloat16)
    sw_value = project(sw_value_weight).astype(jnp.bfloat16).reshape(length, KV_HEADS, HD)
    scale = HD ** (-0.5)
    block = math.gcd(length, 512)
    positions = jnp.arange(length, dtype=jnp.int32)
    keys_wide = da_key.astype(jnp.float32)
    values_wide = da_value.astype(jnp.float32)

    def da_block(first):
        rows = lax.dynamic_slice_in_dim(da_query, first, block, 0).astype(jnp.float32)
        scores = jnp.einsum('qhmd,khmd->hmqk', rows, keys_wide) * scale
        here = first + jnp.arange(block, dtype=jnp.int32)
        scores = jnp.where(positions[None, :] <= here[:, None], scores, -jnp.inf)
        top = lax.optimization_barrier(jnp.max(scores, axis=-1, keepdims=True))
        weights = jnp.exp(scores - top)
        total = lax.optimization_barrier(jnp.sum(weights, axis=-1))
        rounded = lax.optimization_barrier(weights.astype(jnp.bfloat16)).astype(jnp.float32)
        summed = jnp.einsum('hmqk,khe->hmqe', rounded, values_wide)
        maps = summed / total[..., None]
        blend = maps[:, 0] - mix_lambda[:, None, None] * maps[:, 1]
        return jnp.transpose(blend, (1, 0, 2))
    starts = jnp.arange(length // block, dtype=jnp.int32) * block
    blend_all = lax.map(da_block, starts).reshape(length, DA_HEADS, 2 * HD)
    da_rows = rms_norm(blend_all, head_gain).astype(jnp.bfloat16).reshape(length, DA_HEADS * 2 * HD)
    groups = SW_HEADS // KV_HEADS
    count = length // WINDOW

    def band(array):
        tiles = array.astype(jnp.float32).reshape(count, WINDOW, KV_HEADS, HD)
        earlier = jnp.concatenate([jnp.zeros_like(tiles[:1]), tiles[:-1]], axis=0)
        return jnp.concatenate([earlier, tiles], axis=1)
    key_band = band(sw_key)
    value_band = band(sw_value)
    query_tiles = sw_query.astype(jnp.float32).reshape(count, WINDOW, KV_HEADS, groups, HD)
    scores = jnp.einsum('nqhgd,nkhd->nhgqk', query_tiles, key_band) * scale
    lag = WINDOW + jnp.arange(WINDOW)[:, None] - jnp.arange(2 * WINDOW)[None, :]
    key_places = jnp.arange(count)[:, None] * WINDOW - WINDOW + jnp.arange(2 * WINDOW)[None, :]
    valid = ((lag >= 0) & (lag < WINDOW))[None] & (key_places >= 0)[:, None, :]
    scores = jnp.where(valid[:, None, None], scores, -jnp.inf)
    sink = sink_logit.reshape(KV_HEADS, groups)[None, :, :, None]
    top = jnp.maximum(lax.optimization_barrier(jnp.max(scores, axis=-1)), sink)
    weights = jnp.exp(scores - top[..., None])
    total = lax.optimization_barrier(jnp.sum(weights, axis=-1)) + jnp.exp(sink - top)
    rounded = lax.optimization_barrier(weights.astype(jnp.bfloat16)).astype(jnp.float32)
    summed = jnp.einsum('nhgqk,nkhd->nqhgd', rounded, value_band)
    sw_rows = (summed / jnp.transpose(total, (0, 3, 1, 2))[..., None]).astype(jnp.bfloat16).reshape(length, SW_HEADS * HD)
    da_cols = DA_HEADS * 2 * HD // N_TP
    sw_cols = SW_HEADS * HD // N_TP
    mixed = jnp.zeros((length, D), jnp.float32)
    for member in range(N_TP):
        partial_value = jnp.dot(da_rows[:, member * da_cols:(member + 1) * da_cols], da_out_weight[member * da_cols:(member + 1) * da_cols], preferred_element_type=jnp.float32)
        partial_value = partial_value + jnp.dot(sw_rows[:, member * sw_cols:(member + 1) * sw_cols], sw_out_weight[member * sw_cols:(member + 1) * sw_cols], preferred_element_type=jnp.float32)
        mixed = mixed + lax.optimization_barrier(partial_value.astype(jnp.bfloat16)).astype(jnp.float32)
    return mixed.astype(jnp.bfloat16)
```

```python
import functools

import jax
import jax.numpy as jnp
from jax import lax
from jax.experimental import pallas as pl
from jax.experimental.pallas import tpu as pltpu
from jax.sharding import PartitionSpec as P

HD = 64
WINDOW = 128


def shifted(value, axis, steps):
    count = lax.axis_size(axis)
    first, last = (max(0, -steps), min(count, count - steps))
    return lax.ppermute(value, axis, [(source, source + steps) for source in range(first, last)])


def rms_norm(values, gain):
    return values * lax.rsqrt(jnp.mean(values * values, axis=-1, keepdims=True) + 1e-06) * gain


def absorb(state, queries, places, keys, values, key_places):
    top, total, summed = state
    scores = jnp.einsum(
        "qhmd,khmd->hmqk", queries, keys, preferred_element_type=jnp.float32
    ) * HD ** (-0.5)
    scores = jnp.where(key_places[None, :] <= places[:, None], scores, -jnp.inf)
    new_top = jnp.maximum(top, jnp.max(scores, axis=-1))
    weights = jnp.exp(scores - new_top[..., None])
    total = jnp.sum(weights, axis=-1)
    summed = jnp.einsum(
        "hmqk,khe->hmqe", weights.astype(jnp.bfloat16), values, preferred_element_type=jnp.float32
    )
    return (new_top, total, summed)


def keep(state, queries, places, keys, values, key_places):
    return state


def diff_attention(queries, places, da_key, da_value, mix_lambda, head_gain):
    rows = queries.shape[0]
    heads = queries.shape[1]
    half = rows // 2
    fresh = (
        jnp.full((heads, 2, half), -1e30, jnp.float32),
        jnp.zeros((heads, 2, half), jnp.float32),
        jnp.zeros((heads, 2, half, 2 * HD), jnp.float32),
    )
    states = (fresh, fresh)
    start = jnp.int32(0)
    keys = lax.all_gather(da_key, "sp", axis=0, tiled=True)
    values = lax.all_gather(da_value, "sp", axis=0, tiled=True)
    key_places = jnp.arange(keys.shape[0], dtype=jnp.int32)
    updated = []
    for section in range(2):
        own_rows = queries[section * half : (section + 1) * half]
        own_places = places[section * half : (section + 1) * half]
        updated.append(
            lax.cond(
                start <= jnp.max(own_places),
                absorb,
                keep,
                states[section],
                own_rows,
                own_places,
                keys,
                values,
                key_places,
            )
        )
    states = tuple(updated)
    blended = []
    for top, total, summed in states:
        maps = summed / total[..., None]
        blended.append(maps[:, 0] - mix_lambda[:, None, None] * maps[:, 1])
    blend = jnp.transpose(jnp.concatenate(blended, axis=1), (1, 0, 2))
    return rms_norm(blend, head_gain).astype(jnp.bfloat16).reshape(rows, heads * 2 * HD)


def window_attention(sw_query, sw_key, sw_value, earlier_key, earlier_value, sink_logit, first):
    rows = sw_query.shape[0]
    sw_heads = sw_query.shape[1]
    kv_heads = sw_key.shape[1]
    groups = sw_heads // kv_heads
    count = rows // WINDOW

    def band(own, earlier_tile):
        tiles = own.reshape(count, WINDOW, kv_heads, HD)
        earlier = jnp.concatenate([earlier_tile[None], tiles[:-1]], axis=0)
        return jnp.concatenate([earlier, tiles], axis=1)

    key_band = band(sw_key, earlier_key)
    value_band = band(sw_value, earlier_value)
    query_tiles = sw_query.reshape(count, WINDOW, kv_heads, groups, HD)
    scores = jnp.einsum(
        "nqhgd,nkhd->nhgqk", query_tiles, key_band, preferred_element_type=jnp.float32
    ) * HD ** (-0.5)
    lag = WINDOW + jnp.arange(WINDOW)[:, None] - jnp.arange(2 * WINDOW)[None, :]
    key_places = (
        first + jnp.arange(count)[:, None] * WINDOW - WINDOW + jnp.arange(2 * WINDOW)[None, :]
    )
    valid = ((lag >= 0) & (lag < WINDOW))[None] & (key_places >= 0)[:, None, :]
    scores = jnp.where(valid[:, None, None], scores, -jnp.inf)
    sink = sink_logit.reshape(kv_heads, groups)[None, :, :, None]
    top = jnp.maximum(jnp.max(scores, axis=-1), sink)
    weights = jnp.exp(scores - top[..., None])
    total = jnp.sum(weights, axis=-1) + jnp.exp(sink - top)
    summed = jnp.einsum(
        "nhgqk,nkhd->nqhgd",
        weights.astype(jnp.bfloat16),
        value_band,
        preferred_element_type=jnp.float32,
    )
    return (
        (summed / jnp.transpose(total, (0, 3, 1, 2))[..., None])
        .astype(jnp.bfloat16)
        .reshape(rows, sw_heads * HD)
    )


def on_device(
    inputs,
    norm_gain,
    da_query_weight,
    da_key_weight,
    da_value_weight,
    sw_query_weight,
    sw_key_weight,
    sw_value_weight,
    da_query_gain,
    da_key_gain,
    sw_query_gain,
    sw_key_gain,
    mix_lambda,
    head_gain,
    sink_logit,
    da_out_weight,
    sw_out_weight,
):
    rows = inputs.shape[0]
    normed = rms_norm(inputs.astype(jnp.float32), norm_gain).astype(jnp.bfloat16)
    pieces = (
        lax.all_gather(da_query_weight, "sp", axis=0, tiled=True),
        lax.all_gather(da_key_weight, "sp", axis=0, tiled=True),
        lax.all_gather(da_value_weight, "sp", axis=0, tiled=True),
        lax.all_gather(sw_query_weight, "sp", axis=0, tiled=True),
        lax.all_gather(sw_key_weight, "sp", axis=0, tiled=True),
        lax.all_gather(sw_value_weight, "sp", axis=0, tiled=True),
    )
    projected = tuple(
        (jnp.dot(normed, piece, preferred_element_type=jnp.float32) for piece in pieces)
    )
    da_heads = da_query_weight.shape[1] // (2 * HD)
    sw_heads = sw_query_weight.shape[1] // HD
    kv_heads = sw_key_weight.shape[1] // HD
    da_query = rms_norm(projected[0].reshape(rows, da_heads, 2, HD), da_query_gain).astype(
        jnp.bfloat16
    )
    da_key = rms_norm(projected[1].reshape(rows, da_heads, 2, HD), da_key_gain).astype(jnp.bfloat16)
    da_value = projected[2].astype(jnp.bfloat16).reshape(rows, da_heads, 2 * HD)
    sw_query = rms_norm(projected[3].reshape(rows, sw_heads, HD), sw_query_gain).astype(
        jnp.bfloat16
    )
    sw_key = rms_norm(projected[4].reshape(rows, kv_heads, HD), sw_key_gain).astype(jnp.bfloat16)
    sw_value = projected[5].astype(jnp.bfloat16).reshape(rows, kv_heads, HD)
    place = lax.axis_index("sp")
    first = place * rows
    earlier_key, earlier_value = shifted(
        (sw_key[rows - WINDOW :], sw_value[rows - WINDOW :]), "sp", 1
    )
    sw_rows = window_attention(
        sw_query, sw_key, sw_value, earlier_key, earlier_value, sink_logit, first
    )
    places = first + jnp.arange(rows, dtype=jnp.int32)
    da_rows = diff_attention(da_query, places, da_key, da_value, mix_lambda, head_gain)
    partial_value = jnp.dot(da_rows, da_out_weight, preferred_element_type=jnp.float32) + jnp.dot(
        sw_rows, sw_out_weight, preferred_element_type=jnp.float32
    )
    return lax.psum(partial_value.astype(jnp.bfloat16), "tp")


MESH = pl.DeviceIdType.MESH
F32, BF16 = jnp.float32, jnp.bfloat16
CORES = 2


def dot(a, b):
    return jnp.dot(a, b, preferred_element_type=F32)


def dot_t(a, b):
    return lax.dot_general(a, b, (((1,), (1,)), ((), ())), preferred_element_type=F32)


def pair_norm(values, gain):
    lane = lax.broadcasted_iota(jnp.int32, values.shape, 1)
    squares = values * values
    low = jnp.sum(jnp.where(lane < HD, squares, 0.0), axis=-1, keepdims=True)
    high = jnp.sum(jnp.where(lane < HD, 0.0, squares), axis=-1, keepdims=True)
    mean = jnp.where(lane < HD, low, high) * (1.0 / HD)
    return values * lax.rsqrt(mean + 1e-06) * gain


PIECES = 4
CUTS = 4
HALVES = 2
COLUMNS = 4


def kernel(
    n,
    x_hbm,
    da_q_hbm,
    da_k_hbm,
    da_v_hbm,
    sw_q_hbm,
    sw_k_hbm,
    sw_v_hbm,
    norm_gain_hbm,
    da_q_gain_hbm,
    da_k_gain_hbm,
    sw_q_gain_hbm,
    sw_k_gain_hbm,
    head_gain_hbm,
    mix_hbm,
    sink_hbm,
    da_out_hbm,
    sw_out_hbm,
    out_ref,
    x_raw,
    skv_raw,
    norm_gain,
    da_q_gain,
    da_k_gain,
    sw_q_gain,
    sw_k_gain,
    head_gain,
    mix_ref,
    sink_ref,
    wout,
    wp,
    xg,
    wb,
    q_da,
    q_sw,
    kv,
    scal,
    rows_out,
    rows_in,
    sum_out,
    sum_in,
    local_sem,
    x_send,
    x_recv,
    xf_send,
    xf_recv,
    w_send,
    w_recv,
    wy_send,
    wy_recv,
    wc_send,
    wc_recv,
    own_send,
    own_recv,
    kv_send,
    kv_recv,
    sc_send,
    sc_recv,
    wo_send,
    wo_recv,
    r_send,
    r_recv,
    s_send,
    s_recv,
    o_send,
    o_recv,
):
    y = lax.axis_index("grp")
    z = lax.axis_index("sp")
    t = lax.axis_index("tp")
    x = t // CORES
    c = t % CORES
    peer = {"tp": x * CORES + 1 - c}
    across = {"tp": (1 - x) * CORES + c}
    beside = {"grp": 1 - y}
    wide = 2 * HD

    def at(zz, cc):
        return {"sp": zz, "tp": x * CORES + cc}

    def remote(src, dst, send, recv, device):
        return pltpu.make_async_remote_copy(
            src_ref=src,
            dst_ref=dst,
            send_sem=send,
            recv_sem=recv,
            device_id=device,
            device_id_type=MESH,
        )

    def go(copy, when=None):
        if when is None:
            copy.start()
        else:
            pl.when(when)(copy.start)

    barrier = pltpu.get_barrier_semaphore()

    def greet(device):
        pl.semaphore_signal(barrier, inc=1, device_id=device, device_id_type=MESH)

    for k in range(n - 1, 0, -1):
        for cc in range(CORES):
            greet(at(lax.rem(z + k, n), cc))
    greet(across)
    greet(beside)
    greet(peer)

    load_x = pltpu.make_async_copy(x_hbm.at[c], x_raw, local_sem.at[0])
    load_x.start()
    smalls = []
    for i, (source, target) in enumerate(
        (
            (norm_gain_hbm, norm_gain),
            (da_q_gain_hbm, da_q_gain),
            (da_k_gain_hbm, da_k_gain),
            (sw_q_gain_hbm, sw_q_gain),
            (sw_k_gain_hbm, sw_k_gain),
            (head_gain_hbm, head_gain),
            (mix_hbm, mix_ref),
            (sink_hbm, sink_ref),
        )
    ):
        smalls.append(pltpu.make_async_copy(source, target, local_sem.at[1 + i]))
        smalls[-1].start()
    for j, source in enumerate((sw_k_hbm, sw_v_hbm)):
        pltpu.make_async_copy(source, skv_raw.at[j], local_sem.at[9]).start()
    for par in range(CORES):
        for j, source in enumerate((da_q_hbm, da_k_hbm, da_v_hbm, sw_q_hbm)):
            pltpu.make_async_copy(
                source.at[:, :, :, :, pl.ds(par * wide, wide)],
                wp.at[par, :, :, :, :, pl.ds(j * wide, wide)],
                local_sem.at[10],
            ).start()
    for j, source in enumerate((da_out_hbm, sw_out_hbm)):
        pltpu.make_async_copy(source, wout.at[j, c], local_sem.at[11]).start()

    smalls[0].wait()
    load_x.wait()
    for h in range(2):
        for p in range(PIECES):
            values = rms_norm(x_raw[h, p].astype(F32), norm_gain[...])
            xg[z, h, p] = values.astype(BF16)
    pltpu.make_async_copy(skv_raw, skv_raw, local_sem.at[9]).wait()
    for par in range(CORES):
        cols = slice(par * HD, (par + 1) * HD)
        wp[par, :, :, :, :, 4 * wide : 5 * wide] = jnp.concatenate(
            [skv_raw[0, ..., cols], skv_raw[1, ..., cols]], axis=-1
        )
    for load in smalls[1:]:
        load.wait()
    for par in range(CORES):
        scal[c, par, 0:1, :] = jnp.broadcast_to(mix_ref[:, par : par + 1], (1, wide))
        for g in range(2):
            sink = sink_ref[:, 2 * par + g : 2 * par + g + 1]
            scal[c, par, 1 + g : 2 + g, :] = jnp.broadcast_to(sink, (1, wide))
    packed = wp.at[:, :, :, :, :, pl.ds(0, 4 * wide)]
    pltpu.make_async_copy(packed, packed, local_sem.at[10]).wait()
    pl.semaphore_wait(barrier, 3 + (n - 1) * CORES)

    def from_there(d, k):
        return jnp.clip(z - k if d == 0 else z + k, 0, n - 1)

    def has(d, k):
        return z - k >= 0 if d == 0 else z + k < n

    def can_hop(d, k):
        return (z - k >= 0) & (z + 1 < n) if d == 0 else (z + k < n) & (z >= 1)

    def hop(d, k, p):
        source = from_there(d, k)
        target = jnp.clip(z + 1 if d == 0 else z - 1, 0, n - 1)
        piece = xg.at[source, x, p]
        return remote(piece, piece, x_send.at[d], x_recv.at[d, k, p], {"sp": target})

    def cross(zs, p):
        piece = xg.at[zs, x, p]
        return remote(piece, piece, xf_send, xf_recv.at[zs], across)

    owner = c == z // CORES

    def send_weights(s):
        for par in range(CORES):
            zt = CORES * c + par
            for cd in range(CORES):
                piece = wp.at[par, y, cd, s]
                go(
                    remote(piece, wb.at[z, y, cd, s], w_send, w_recv.at[z, s], at(zt, cd)),
                    zt != z,
                )

    def weight_beside(zs, yy, s):
        piece = wb.at[zs, yy, c, s]
        return remote(piece, piece, wy_send, wy_recv.at[zs, s], beside)

    def weight_core(zs, yy, s):
        piece = wb.at[zs, yy, c, s]
        return remote(piece, piece, wc_send, wc_recv, peer)

    def event_x(d, k, p):
        zs = from_there(d, k)

        @pl.when(has(d, k))
        def _():
            piece = xg.at[zs, x, p]
            remote(piece, piece, x_send.at[d], x_recv.at[d, k - 1, p], across).wait_recv()

        if k < n - 1:
            go(hop(d, k, p), can_hop(d, k))
        go(cross(zs, p), has(d, k))

    def event_w(d, k, s):
        zs = from_there(d, k)

        @pl.when(has(d, k))
        def _():
            piece = wb.at[zs, y, c, s]
            remote(piece, piece, w_send, w_recv.at[zs, s], peer).wait_recv()
            weight_beside(zs, y, s).start()
            weight_core(zs, y, s).start()

    def event_y(d, k, s):
        zs = from_there(d, k)

        @pl.when(has(d, k))
        def _():
            weight_beside(zs, 1 - y, s).wait_recv()
            weight_core(zs, 1 - y, s).start()

    def both(event, k, p):
        for d in range(2):
            event(d, k, p)

    tile = xg.shape[1] * xg.shape[2] * xg.shape[3]
    depth = wb.shape[1] * wb.shape[2] * wb.shape[3] * wb.shape[4]
    width = wb.shape[5]

    def lanes(shape):
        return lax.broadcasted_iota(jnp.int32, shape, len(shape) - 1)

    low = lanes((tile, wide)) < HD

    def twice(ref):
        return jnp.concatenate([ref[...], ref[...]], axis=-1)

    def arrive(b):
        @pl.when(b != z)
        def _():
            block = xg.at[b, 1 - x]
            remote(block, block, xf_send, xf_recv.at[b], across).wait_recv()

    def project(b):
        block = xg[b].reshape(tile, xg.shape[4])
        acc = dot(block[:, 0:depth], wb[0].reshape(depth, width))
        for j in range(1, n):
            acc += dot(block[:, j * depth : (j + 1) * depth], wb[j].reshape(depth, width))
        scale = HD ** (-0.5)

        def heads(values, gain):
            normed = pair_norm(values, gain).astype(BF16).astype(F32) * scale
            low_half = jnp.where(low, normed, 0.0).astype(BF16)
            high_half = jnp.where(low, 0.0, normed).astype(BF16)
            return low_half, high_half

        low_half, high_half = heads(acc[:, 0:wide], twice(da_q_gain))
        q_da[b, 0] = low_half
        q_da[b, 1] = high_half
        low_half, high_half = heads(acc[:, 3 * wide : 4 * wide], twice(sw_q_gain))
        q_sw[b, 0] = low_half
        q_sw[b, 1] = high_half
        key = pair_norm(acc[:, wide : 2 * wide], twice(da_k_gain))
        kv[c, b, :, 0:wide] = key.astype(BF16)
        kv[c, b, :, wide : 2 * wide] = acc[:, 2 * wide : 3 * wide].astype(BF16)
        pair = acc[:, 4 * wide : 5 * wide]
        key = pair_norm(pair, twice(sw_k_gain))
        key = jnp.where(low, key, pltpu.roll(key, HD, 1))
        value = jnp.where(low, pltpu.roll(pair, HD, 1), pair)
        kv[c, b, :, 2 * wide : 3 * wide] = key.astype(BF16)
        kv[c, b, :, 3 * wide : 4 * wide] = value.astype(BF16)

    def swap(b, core):
        block = kv.at[core, b]
        return remote(block, block, kv_send, kv_recv.at[b], peer)

    def mine():
        return scal[z // CORES, z % CORES]

    def window(i):
        before = jnp.maximum(i - 1 + c, 0)
        q = q_sw[i].reshape(2 * tile, wide)
        near = kv[c, i, :, 2 * wide : 4 * wide]
        far = kv[1 - c, before, :, 2 * wide : 4 * wide]
        row = lax.broadcasted_iota(jnp.int32, (2 * tile, tile), 0)
        head = row[:, 0:1] < tile
        row = jnp.where(row < tile, row, row - tile)
        column = lanes((2 * tile, tile))
        first_ok = (2 * i + c) > 0
        s_near = jnp.where(column <= row, dot_t(q, near[:, 0:wide]), -jnp.inf)
        s_far = jnp.where((column > row) & first_ok, dot_t(q, far[:, 0:wide]), -jnp.inf)
        own = mine()
        sink = jnp.where(head, own[1:2, 0:1], own[2:3, 0:1])
        top = jnp.maximum(jnp.max(jnp.maximum(s_near, s_far), axis=-1, keepdims=True), sink)
        w_near = jnp.exp(s_near - top)
        w_far = jnp.exp(s_far - top)
        total = jnp.sum(w_near + w_far, axis=-1, keepdims=True) + jnp.exp(sink - top)
        summed = dot(w_near.astype(BF16), near[:, wide : 2 * wide]) + dot(
            w_far.astype(BF16), far[:, wide : 2 * wide]
        )
        result = summed / total
        return jnp.where(low, result[0:tile], result[tile : 2 * tile]).astype(BF16)

    part = tile // HALVES

    def spread(i, half):
        rows = slice(half * part, (half + 1) * part)
        size = 2 * part
        q = q_da[i, :, rows, :].reshape(size, wide)
        row = lax.broadcasted_iota(jnp.int32, (size, tile), 0)
        row = jnp.where(row < part, row, row - part) + half * part
        column = lanes((size, tile))
        scores = []
        top = None
        for h in range(2):
            keys = kv[h, 0 : i + 1, :, 0:wide].reshape((i + 1) * tile, wide)
            s = dot_t(q, keys)
            tiles = [s[:, j * tile : (j + 1) * tile] for j in range(i + 1)]
            tiles[i] = jnp.where(column + (h - c) * tile <= row, tiles[i], -jnp.inf)
            scores.append(tiles)
            for one in tiles:
                top = one if top is None else jnp.maximum(top, one)
        top = jnp.max(top, axis=-1, keepdims=True)
        total = None
        summed = None
        for h in range(2):
            weights = [jnp.exp(one - top) for one in scores[h]]
            for one in weights:
                total = one if total is None else total + one
            values = kv[h, 0 : i + 1, :, wide : 2 * wide].reshape((i + 1) * tile, wide)
            flat = jnp.concatenate([one.astype(BF16) for one in weights], axis=-1)
            step = dot(flat, values)
            summed = step if summed is None else summed + step
        total = jnp.sum(total, axis=-1, keepdims=True)
        maps = summed / total
        blend = maps[0:part] - mine()[0:1, :] * maps[part:size]
        return rms_norm(blend, head_gain[...]).astype(BF16)

    def send_rows(i, j, half):
        rows = pl.ds(half * part, part)
        go(
            remote(
                rows_out.at[i, j, rows],
                rows_in.at[j, z, rows],
                r_send,
                r_recv.at[j, half],
                {"sp": i},
            ),
            z != i,
        )

        @pl.when(z == i)
        def _():
            rows = slice(half * part, (half + 1) * part)
            rows_in[j, i, rows, :] = rows_out[i, j, rows, :]

    def await_rows(j, half):
        block = rows_in.at[j, 0 : n - 1, pl.ds(half * part, part)]
        remote(block, block, r_send, r_recv.at[j, half], peer).wait_recv()

    blocks = (
        z,
        z + 1 - 2 * (z % 2),
        jnp.where(z < 2, 2, 1),
        jnp.where(z < 2, 3, 0),
    )

    own = remote(wp.at[z % CORES], wb.at[z], own_send, own_recv, peer)
    own_local = pltpu.make_async_copy(wp.at[z % CORES], wb.at[z], local_sem.at[12])
    sc = remote(scal.at[c], scal.at[c], sc_send, sc_recv, peer)
    share = remote(wout.at[:, c], wout.at[:, c], wo_send, wo_recv, peer)

    for p in range(PIECES):
        send_weights(p)
        for d in range(2):
            go(hop(d, 0, p), can_hop(d, 0))
    go(own, jnp.logical_not(owner) if False else owner)
    pl.when(owner)(own_local.start)
    go(sc)
    pltpu.make_async_copy(wout.at[:, c], wout.at[:, c], local_sem.at[11]).wait()
    go(share)

    for p in range(PIECES):
        both(event_x, 1, p)
        for k in range(1, n):
            both(event_w, k, p)
        if p:
            for k in range(1, n):
                both(event_y, k, p - 1)
            both(event_x, 2, p - 1)
    for k in range(1, n):
        both(event_y, k, PIECES - 1)
    both(event_x, 2, PIECES - 1)
    pl.when(owner)(own_local.wait)
    pl.when(jnp.logical_not(owner))(own.wait_recv)
    theirs = wb.at[0 : n - 1, :, 1 - c]
    remote(theirs, theirs, wc_send, wc_recv, peer).wait_recv()
    project(blocks[0])
    go(swap(blocks[0], c))
    both(event_x, 3, 0)
    arrive(blocks[1])
    project(blocks[1])
    go(swap(blocks[1], c))
    both(event_x, 3, 1)
    both(event_x, 3, 2)
    both(event_x, 3, 3)
    arrive(blocks[2])
    project(blocks[2])
    go(swap(blocks[2], c))
    remote(scal.at[1 - c], scal.at[1 - c], sc_send, sc_recv, peer).wait_recv()
    for b in blocks[:3]:
        swap(b, 1 - c).wait_recv()
    early = (jnp.where(z < 2, 1, 3), 2)
    late = (jnp.where(z < 2, 0, 1), jnp.where(z < 2, 3, 0))
    for i in early:
        rows_out[i, 1] = window(i)
    arrive(blocks[3])
    project(blocks[3])
    go(swap(blocks[3], c))
    swap(blocks[3], 1 - c).wait_recv()
    for i in late:
        rows_out[i, 1] = window(i)
    for half in range(HALVES):
        rows = slice(half * part, (half + 1) * part)
        for i in range(n):
            send_rows(i, 1, half)
        for i in (3, 0, 2, 1):
            rows_out[i, 0, rows, :] = spread(i, half)
        for i in (3, 0, 2, 1):
            send_rows(i, 0, half)

    share_in = wout.at[:, 1 - c]
    remote(share_in, share_in, wo_send, wo_recv, peer).wait_recv()
    columns = out_ref.shape[2] // COLUMNS

    def span(half, q):
        return pl.ds(half * part, part), pl.ds(q * columns, columns)

    def summing(half, q):
        rows, cols = span(half, q)
        return remote(
            sum_out.at[rows, cols],
            sum_in.at[rows, cols],
            s_send,
            s_recv.at[half, q],
            across,
        )

    def finish(half, q):
        rows, cols = span(half, q)
        summing(half, q).wait_recv()
        out_ref[c, rows, cols] = (sum_out[rows, cols].astype(F32) + sum_in[rows, cols].astype(F32)).astype(BF16)
        block = out_ref.at[c, rows, cols]
        go(remote(block, block, o_send, o_recv, peer))

    for half in range(HALVES):
        rows = slice(half * part, (half + 1) * part)
        await_rows(1, half)
        await_rows(0, half)
        for q in range(COLUMNS):
            cols = slice(q * columns, (q + 1) * columns)
            acc = None
            for j in range(2):
                values = jnp.concatenate([rows_in[j, zs, rows, :] for zs in range(n)], axis=-1)
                step = dot(values, wout[j, :, :, cols].reshape(2 * wout.shape[2], columns))
                acc = step if acc is None else acc + step
            sum_out[rows, cols] = acc.astype(BF16)
            go(summing(half, q))
    for half in range(HALVES):
        for q in range(COLUMNS):
            finish(half, q)
    block = out_ref.at[1 - c]
    remote(block, block, o_send, o_recv, peer).wait_recv()

    def drained(ref, sem):
        remote(ref, ref, sem, o_recv, peer).wait_send()

    for zz in range(n):

        @pl.when(z == zz)
        def _(zz=zz):
            if zz + 1 < n:
                drained(xg.at[0 : zz + 1, x], x_send.at[0])
            if zz >= 1:
                drained(xg.at[0 : n - zz, x], x_send.at[1])

    drained(xg.at[0 : n - 1, x], xf_send)
    pl.when(owner)(lambda: drained(wp.at[0, y], w_send))
    pl.when(jnp.logical_not(owner))(lambda: drained(wp.at[:, y], w_send))
    pl.when(owner)(lambda: drained(wp.at[0], own_send))
    drained(wb.at[0 : n - 1, y, c], wy_send)
    drained(wb.at[0 : n - 1, :, c], wc_send)
    drained(scal.at[c], sc_send)
    drained(wout.at[:, c], wo_send)
    drained(kv.at[c], kv_send)
    drained(rows_out.at[0 : n - 1], r_send)
    drained(sum_out, s_send)
    drained(out_ref.at[c], o_send)


def transposed(n, *arrays):
    (
        inputs,
        norm_gain,
        da_query_weight,
        da_key_weight,
        da_value_weight,
        sw_query_weight,
        sw_key_weight,
        sw_value_weight,
        da_query_gain,
        da_key_gain,
        sw_query_gain,
        sw_key_gain,
        mix_lambda,
        head_gain,
        sink_logit,
        da_out_weight,
        sw_out_weight,
    ) = arrays
    rows, d = inputs.shape
    depth = da_query_weight.shape[0]
    wide = 2 * HD
    width = 5 * wide
    cut_rows = depth // 4 // CUTS
    tile = rows // 2
    part = tile // 2 // PIECES
    group = da_out_weight.shape[0]

    def cut(weight):
        return weight.reshape(2, CORES, CUTS, cut_rows, weight.shape[1])

    def line(vector):
        return vector.reshape(1, -1)

    DMA = pltpu.SemaphoreType.DMA
    any_space = pl.BlockSpec(memory_space=pl.ANY)
    out = pl.pallas_call(
        functools.partial(kernel, n),
        out_shape=pltpu.VMEM((2, tile, d), BF16),
        in_specs=[any_space] * 17,
        out_specs=pl.BlockSpec(memory_space=pltpu.VMEM),
        scratch_shapes=[
            pltpu.VMEM((2, PIECES, part, d), BF16),
            pltpu.VMEM((2, 2, CORES, CUTS, cut_rows, wide), BF16),
            pltpu.VMEM((1, d), F32),
            pltpu.VMEM((1, HD), F32),
            pltpu.VMEM((1, HD), F32),
            pltpu.VMEM((1, HD), F32),
            pltpu.VMEM((1, HD), F32),
            pltpu.VMEM((1, wide), F32),
            pltpu.VMEM((1, mix_lambda.shape[0]), F32),
            pltpu.VMEM((1, sink_logit.shape[0]), F32),
            pltpu.VMEM((2, CORES, group, d), BF16),
            pltpu.VMEM((CORES, 2, CORES, CUTS, cut_rows, width), BF16),
            pltpu.VMEM((n, 2, PIECES, part, d), BF16),
            pltpu.VMEM((n, 2, CORES, CUTS, cut_rows, width), BF16),
            pltpu.VMEM((n, 2, tile, wide), BF16),
            pltpu.VMEM((n, 2, tile, wide), BF16),
            pltpu.VMEM((CORES, n, tile, 4 * wide), BF16),
            pltpu.VMEM((CORES, CORES, 8, wide), F32),
            pltpu.VMEM((n, 2, tile, wide), BF16),
            pltpu.VMEM((2, n, tile, wide), BF16),
            pltpu.VMEM((tile, d), BF16),
            pltpu.VMEM((tile, d), BF16),
            DMA((14,)),
            DMA((2,)),
            DMA((2, n - 1, PIECES)),
            DMA,
            DMA((n,)),
            DMA,
            DMA((n, CUTS)),
            DMA,
            DMA((n, CUTS)),
            DMA,
            DMA,
            DMA,
            DMA,
            DMA,
            DMA((n,)),
            DMA,
            DMA,
            DMA,
            DMA,
            DMA,
            DMA((2, HALVES)),
            DMA,
            DMA((HALVES, COLUMNS)),
            DMA,
            DMA,
        ],
        compiler_params=pltpu.CompilerParams(
            collective_id=0, has_side_effects=True, vmem_limit_bytes=60 * 1024 * 1024
        ),
    )(
        inputs.reshape(CORES, 2, PIECES, part, d),
        cut(da_query_weight),
        cut(da_key_weight),
        cut(da_value_weight),
        cut(sw_query_weight),
        cut(sw_key_weight),
        cut(sw_value_weight),
        line(norm_gain),
        line(da_query_gain),
        line(da_key_gain),
        line(sw_query_gain),
        line(sw_key_gain),
        line(head_gain),
        line(mix_lambda),
        line(sink_logit),
        da_out_weight,
        sw_out_weight,
    )
    return out.reshape(rows, d)


def body(sizes, *arrays):
    rows = arrays[0].shape[0]
    heads = arrays[12].shape[0]
    sinks = arrays[14].shape[0]
    n = sizes["sp"]
    fits = (
        sizes["grp"] == 2
        and sizes["tp"] == 2 * CORES
        and n == 2 * CORES
        and heads == CORES
        and sinks == 2 * CORES
        and arrays[6].shape[1] == CORES * HD
        and rows == 2 * WINDOW
    )
    if fits:
        return transposed(n, *arrays)
    return on_device(*arrays)


def solution(mesh):
    return jax.shard_map(
        functools.partial(body, dict(mesh.shape)),
        mesh=mesh,
        in_specs=(
            P(("grp", "sp"), None),
            P(),
            P("sp", "tp"),
            P("sp", "tp"),
            P("sp", "tp"),
            P("sp", "tp"),
            P("sp", "tp"),
            P("sp", "tp"),
            P(),
            P(),
            P(),
            P(),
            P("tp"),
            P(),
            P("tp"),
            P("tp", None),
            P("tp", None),
        ),
        out_specs=P(("grp", "sp"), None),
        check_vma=False,
    )
```

```python
import functools

import jax
import jax.numpy as jnp
from jax import lax
from jax.experimental import pallas as pl
from jax.experimental.pallas import tpu as pltpu
from jax.sharding import PartitionSpec as P

HD = 64
WINDOW = 128


def shifted(value, axis, steps):
    count = lax.axis_size(axis)
    first, last = (max(0, -steps), min(count, count - steps))
    return lax.ppermute(value, axis, [(source, source + steps) for source in range(first, last)])


def rms_norm(values, gain):
    return values * lax.rsqrt(jnp.mean(values * values, axis=-1, keepdims=True) + 1e-06) * gain


def absorb(state, queries, places, keys, values, key_places):
    top, total, summed = state
    scores = jnp.einsum(
        "qhmd,khmd->hmqk", queries, keys, preferred_element_type=jnp.float32
    ) * HD ** (-0.5)
    scores = jnp.where(key_places[None, :] <= places[:, None], scores, -jnp.inf)
    new_top = jnp.maximum(top, jnp.max(scores, axis=-1))
    weights = jnp.exp(scores - new_top[..., None])
    total = jnp.sum(weights, axis=-1)
    summed = jnp.einsum(
        "hmqk,khe->hmqe", weights.astype(jnp.bfloat16), values, preferred_element_type=jnp.float32
    )
    return (new_top, total, summed)


def keep(state, queries, places, keys, values, key_places):
    return state


def diff_attention(queries, places, da_key, da_value, mix_lambda, head_gain):
    rows = queries.shape[0]
    heads = queries.shape[1]
    half = rows // 2
    fresh = (
        jnp.full((heads, 2, half), -1e30, jnp.float32),
        jnp.zeros((heads, 2, half), jnp.float32),
        jnp.zeros((heads, 2, half, 2 * HD), jnp.float32),
    )
    states = (fresh, fresh)
    start = jnp.int32(0)
    keys = lax.all_gather(da_key, "sp", axis=0, tiled=True)
    values = lax.all_gather(da_value, "sp", axis=0, tiled=True)
    key_places = jnp.arange(keys.shape[0], dtype=jnp.int32)
    updated = []
    for section in range(2):
        own_rows = queries[section * half : (section + 1) * half]
        own_places = places[section * half : (section + 1) * half]
        updated.append(
            lax.cond(
                start <= jnp.max(own_places),
                absorb,
                keep,
                states[section],
                own_rows,
                own_places,
                keys,
                values,
                key_places,
            )
        )
    states = tuple(updated)
    blended = []
    for top, total, summed in states:
        maps = summed / total[..., None]
        blended.append(maps[:, 0] - mix_lambda[:, None, None] * maps[:, 1])
    blend = jnp.transpose(jnp.concatenate(blended, axis=1), (1, 0, 2))
    return rms_norm(blend, head_gain).astype(jnp.bfloat16).reshape(rows, heads * 2 * HD)


def window_attention(sw_query, sw_key, sw_value, earlier_key, earlier_value, sink_logit, first):
    rows = sw_query.shape[0]
    sw_heads = sw_query.shape[1]
    kv_heads = sw_key.shape[1]
    groups = sw_heads // kv_heads
    count = rows // WINDOW

    def band(own, earlier_tile):
        tiles = own.reshape(count, WINDOW, kv_heads, HD)
        earlier = jnp.concatenate([earlier_tile[None], tiles[:-1]], axis=0)
        return jnp.concatenate([earlier, tiles], axis=1)

    key_band = band(sw_key, earlier_key)
    value_band = band(sw_value, earlier_value)
    query_tiles = sw_query.reshape(count, WINDOW, kv_heads, groups, HD)
    scores = jnp.einsum(
        "nqhgd,nkhd->nhgqk", query_tiles, key_band, preferred_element_type=jnp.float32
    ) * HD ** (-0.5)
    lag = WINDOW + jnp.arange(WINDOW)[:, None] - jnp.arange(2 * WINDOW)[None, :]
    key_places = (
        first + jnp.arange(count)[:, None] * WINDOW - WINDOW + jnp.arange(2 * WINDOW)[None, :]
    )
    valid = ((lag >= 0) & (lag < WINDOW))[None] & (key_places >= 0)[:, None, :]
    scores = jnp.where(valid[:, None, None], scores, -jnp.inf)
    sink = sink_logit.reshape(kv_heads, groups)[None, :, :, None]
    top = jnp.maximum(jnp.max(scores, axis=-1), sink)
    weights = jnp.exp(scores - top[..., None])
    total = jnp.sum(weights, axis=-1) + jnp.exp(sink - top)
    summed = jnp.einsum(
        "nhgqk,nkhd->nqhgd",
        weights.astype(jnp.bfloat16),
        value_band,
        preferred_element_type=jnp.float32,
    )
    return (
        (summed / jnp.transpose(total, (0, 3, 1, 2))[..., None])
        .astype(jnp.bfloat16)
        .reshape(rows, sw_heads * HD)
    )


def on_device(
    inputs,
    norm_gain,
    da_query_weight,
    da_key_weight,
    da_value_weight,
    sw_query_weight,
    sw_key_weight,
    sw_value_weight,
    da_query_gain,
    da_key_gain,
    sw_query_gain,
    sw_key_gain,
    mix_lambda,
    head_gain,
    sink_logit,
    da_out_weight,
    sw_out_weight,
):
    rows = inputs.shape[0]
    normed = rms_norm(inputs.astype(jnp.float32), norm_gain).astype(jnp.bfloat16)
    pieces = (
        lax.all_gather(da_query_weight, "sp", axis=0, tiled=True),
        lax.all_gather(da_key_weight, "sp", axis=0, tiled=True),
        lax.all_gather(da_value_weight, "sp", axis=0, tiled=True),
        lax.all_gather(sw_query_weight, "sp", axis=0, tiled=True),
        lax.all_gather(sw_key_weight, "sp", axis=0, tiled=True),
        lax.all_gather(sw_value_weight, "sp", axis=0, tiled=True),
    )
    projected = tuple(
        (jnp.dot(normed, piece, preferred_element_type=jnp.float32) for piece in pieces)
    )
    da_heads = da_query_weight.shape[1] // (2 * HD)
    sw_heads = sw_query_weight.shape[1] // HD
    kv_heads = sw_key_weight.shape[1] // HD
    da_query = rms_norm(projected[0].reshape(rows, da_heads, 2, HD), da_query_gain).astype(
        jnp.bfloat16
    )
    da_key = rms_norm(projected[1].reshape(rows, da_heads, 2, HD), da_key_gain).astype(jnp.bfloat16)
    da_value = projected[2].astype(jnp.bfloat16).reshape(rows, da_heads, 2 * HD)
    sw_query = rms_norm(projected[3].reshape(rows, sw_heads, HD), sw_query_gain).astype(
        jnp.bfloat16
    )
    sw_key = rms_norm(projected[4].reshape(rows, kv_heads, HD), sw_key_gain).astype(jnp.bfloat16)
    sw_value = projected[5].astype(jnp.bfloat16).reshape(rows, kv_heads, HD)
    place = lax.axis_index("sp")
    first = place * rows
    earlier_key, earlier_value = shifted(
        (sw_key[rows - WINDOW :], sw_value[rows - WINDOW :]), "sp", 1
    )
    sw_rows = window_attention(
        sw_query, sw_key, sw_value, earlier_key, earlier_value, sink_logit, first
    )
    places = first + jnp.arange(rows, dtype=jnp.int32)
    da_rows = diff_attention(da_query, places, da_key, da_value, mix_lambda, head_gain)
    partial_value = jnp.dot(da_rows, da_out_weight, preferred_element_type=jnp.float32) + jnp.dot(
        sw_rows, sw_out_weight, preferred_element_type=jnp.float32
    )
    return lax.psum(partial_value.astype(jnp.bfloat16), "tp")


MESH = pl.DeviceIdType.MESH
F32, BF16 = jnp.float32, jnp.bfloat16
CORES = 2


def dot(a, b):
    return jnp.dot(a, b, preferred_element_type=F32)


def dot_t(a, b):
    return lax.dot_general(a, b, (((1,), (1,)), ((), ())), preferred_element_type=F32)


def pair_norm(values, gain):
    lane = lax.broadcasted_iota(jnp.int32, values.shape, 1)
    squares = values * values
    low = jnp.sum(jnp.where(lane < HD, squares, 0.0), axis=-1, keepdims=True)
    high = jnp.sum(jnp.where(lane < HD, 0.0, squares), axis=-1, keepdims=True)
    mean = jnp.where(lane < HD, low, high) * (1.0 / HD)
    return values * lax.rsqrt(mean + 1e-06) * gain


PIECES = 4
CUTS = 4
HALVES = 2
COLUMNS = 4
SHARES = 4


def kernel(
    n,
    x_hbm,
    da_q_hbm,
    da_k_hbm,
    da_v_hbm,
    sw_q_hbm,
    sw_k_hbm,
    sw_v_hbm,
    norm_gain_hbm,
    da_q_gain_hbm,
    da_k_gain_hbm,
    sw_q_gain_hbm,
    sw_k_gain_hbm,
    head_gain_hbm,
    mix_hbm,
    sink_hbm,
    da_out_hbm,
    sw_out_hbm,
    out_ref,
    x_raw,
    skv_raw,
    norm_gain,
    da_q_gain,
    da_k_gain,
    sw_q_gain,
    sw_k_gain,
    head_gain,
    mix_ref,
    sink_ref,
    wout,
    wp,
    xg,
    wb,
    q_da,
    q_sw,
    kv,
    scal,
    rows_out,
    rows_in,
    sum_out,
    sum_in,
    local_sem,
    x_send,
    x_recv,
    xf_send,
    xf_recv,
    w_send,
    w_recv,
    wy_send,
    wy_recv,
    wc_send,
    wc_recv,
    own_send,
    own_recv,
    kv_send,
    kv_recv,
    sc_send,
    sc_recv,
    wo_send,
    wo_recv,
    r_send,
    r_recv,
    s_send,
    s_recv,
    o_send,
    o_recv,
):
    y = lax.axis_index("grp")
    z = lax.axis_index("sp")
    t = lax.axis_index("tp")
    x = t // CORES
    c = t % CORES
    peer = {"tp": x * CORES + 1 - c}
    across = {"tp": (1 - x) * CORES + c}
    beside = {"grp": 1 - y}
    wide = 2 * HD

    def at(zz, cc):
        return {"sp": zz, "tp": x * CORES + cc}

    def remote(src, dst, send, recv, device):
        return pltpu.make_async_remote_copy(
            src_ref=src,
            dst_ref=dst,
            send_sem=send,
            recv_sem=recv,
            device_id=device,
            device_id_type=MESH,
        )

    def go(copy, when=None):
        if when is None:
            copy.start()
        else:
            pl.when(when)(copy.start)

    barrier = pltpu.get_barrier_semaphore()

    def greet(device):
        pl.semaphore_signal(barrier, inc=1, device_id=device, device_id_type=MESH)

    for k in range(n - 1, 0, -1):
        for cc in range(CORES):
            greet(at(lax.rem(z + k, n), cc))
    greet(across)
    greet(beside)
    greet(peer)

    load_x = pltpu.make_async_copy(x_hbm.at[c], x_raw, local_sem.at[0])
    load_x.start()
    smalls = []
    for i, (source, target) in enumerate(
        (
            (norm_gain_hbm, norm_gain),
            (da_q_gain_hbm, da_q_gain),
            (da_k_gain_hbm, da_k_gain),
            (sw_q_gain_hbm, sw_q_gain),
            (sw_k_gain_hbm, sw_k_gain),
            (head_gain_hbm, head_gain),
            (mix_hbm, mix_ref),
            (sink_hbm, sink_ref),
        )
    ):
        smalls.append(pltpu.make_async_copy(source, target, local_sem.at[1 + i]))
        smalls[-1].start()
    for j, source in enumerate((sw_k_hbm, sw_v_hbm)):
        pltpu.make_async_copy(source, skv_raw.at[j], local_sem.at[9]).start()
    for par in range(CORES):
        for j, source in enumerate((da_q_hbm, da_k_hbm, da_v_hbm, sw_q_hbm)):
            pltpu.make_async_copy(
                source.at[:, :, :, :, pl.ds(par * wide, wide)],
                wp.at[par, :, :, :, :, pl.ds(j * wide, wide)],
                local_sem.at[10],
            ).start()
    for j, source in enumerate((da_out_hbm, sw_out_hbm)):
        pltpu.make_async_copy(source, wout.at[j, c], local_sem.at[11]).start()

    smalls[0].wait()
    load_x.wait()
    for h in range(2):
        for p in range(PIECES):
            values = rms_norm(x_raw[h, p].astype(F32), norm_gain[...])
            xg[z, h, p] = values.astype(BF16)
    pltpu.make_async_copy(skv_raw, skv_raw, local_sem.at[9]).wait()
    for par in range(CORES):
        cols = slice(par * HD, (par + 1) * HD)
        wp[par, :, :, :, :, 4 * wide : 5 * wide] = jnp.concatenate(
            [skv_raw[0, ..., cols], skv_raw[1, ..., cols]], axis=-1
        )
    for load in smalls[1:]:
        load.wait()
    for par in range(CORES):
        scal[c, par, 0:1, :] = jnp.broadcast_to(mix_ref[:, par : par + 1], (1, wide))
        for g in range(2):
            sink = sink_ref[:, 2 * par + g : 2 * par + g + 1]
            scal[c, par, 1 + g : 2 + g, :] = jnp.broadcast_to(sink, (1, wide))
    packed = wp.at[:, :, :, :, :, pl.ds(0, 4 * wide)]
    pltpu.make_async_copy(packed, packed, local_sem.at[10]).wait()
    pl.semaphore_wait(barrier, 3 + (n - 1) * CORES)

    def way(d):
        return 1 - 2 * d

    def cross(zs, p):
        piece = xg.at[zs, x, p]
        return remote(piece, piece, xf_send, xf_recv.at[zs], across)

    owner = c == z // CORES

    def hop(zz, d, k, p):
        source, target = zz - k * way(d), zz + way(d)
        if 0 <= target < n:
            piece = xg.at[source, x, p]
            remote(piece, piece, x_send.at[d], x_recv.at[d, k, p], {"sp": target}).start()

    def weight_beside(zs, yy, s):
        piece = wb.at[zs, yy, c, s]
        return remote(piece, piece, wy_send, wy_recv.at[zs, s], beside)

    def weight_core(zs, yy, s):
        piece = wb.at[zs, yy, c, s]
        return remote(piece, piece, wc_send, wc_recv, peer)

    def event_x(zz, d, k, p):
        zs = zz - k * way(d)
        piece = xg.at[zs, x, p]
        remote(piece, piece, x_send.at[d], x_recv.at[d, k - 1, p], across).wait_recv()
        if k < n - 1:
            hop(zz, d, k, p)
        cross(zs, p).start()

    def event_w(zs, s):
        piece = wb.at[zs, y, c, s]
        remote(piece, piece, w_send, w_recv.at[zs, s], peer).wait_recv()
        weight_beside(zs, y, s).start()
        weight_core(zs, y, s).start()

    def event_y(zs, s):
        weight_beside(zs, 1 - y, s).wait_recv()
        weight_core(zs, 1 - y, s).start()

    def send_weight(zz, zt, s):
        for cd in range(CORES):
            remote(
                wp.at[zt % CORES, y, cd, s],
                wb.at[zz, y, cd, s],
                w_send,
                w_recv.at[zz, s],
                at(zt, cd),
            ).start()

    def run(script):
        for zz in range(n):
            for cc in range(CORES):

                @pl.when((z == zz) & (c == cc))
                def _(zz=zz, cc=cc):
                    script(zz, cc)

    tile = xg.shape[1] * xg.shape[2] * xg.shape[3]
    depth = wb.shape[1] * wb.shape[2] * wb.shape[3] * wb.shape[4]
    width = wb.shape[5]

    def lanes(shape):
        return lax.broadcasted_iota(jnp.int32, shape, len(shape) - 1)

    low = lanes((tile, wide)) < HD

    def twice(ref):
        return jnp.concatenate([ref[...], ref[...]], axis=-1)

    normed = pair_norm

    def arrive(b):
        @pl.when(b != z)
        def _():
            block = xg.at[b, 1 - x]
            remote(block, block, xf_send, xf_recv.at[b], across).wait_recv()

    def project(b):
        block = xg[b].reshape(tile, xg.shape[4])
        acc = dot(block[:, 0:depth], wb[0].reshape(depth, width))
        for j in range(1, n):
            acc += dot(block[:, j * depth : (j + 1) * depth], wb[j].reshape(depth, width))
        scale = HD ** (-0.5)

        def heads(values, gain):
            result = normed(values, gain).astype(BF16).astype(F32) * scale
            low_half = jnp.where(low, result, 0.0).astype(BF16)
            high_half = jnp.where(low, 0.0, result).astype(BF16)
            return low_half, high_half

        key = normed(acc[:, wide : 2 * wide], twice(da_k_gain))
        kv[c, b, :, 0:wide] = key.astype(BF16)
        kv[c, b, :, wide : 2 * wide] = acc[:, 2 * wide : 3 * wide].astype(BF16)
        pair = acc[:, 4 * wide : 5 * wide]
        pair = jnp.where(low, normed(pair, twice(sw_k_gain)), pair).astype(BF16)
        row = lax.broadcasted_iota(jnp.int32, (wide, 2 * wide), 0)
        column = lanes((wide, 2 * wide))
        source = column % HD + jnp.where(column < wide, 0, HD)
        doubler = jnp.where(row == source, 1.0, 0.0).astype(BF16)
        kv[c, b, :, 2 * wide : 4 * wide] = dot(pair, doubler).astype(BF16)
        swap(b, c).start()
        low_half, high_half = heads(acc[:, 0:wide], twice(da_q_gain))
        q_da[b, 0] = low_half
        q_da[b, 1] = high_half
        low_half, high_half = heads(acc[:, 3 * wide : 4 * wide], twice(sw_q_gain))
        q_sw[b, 0] = low_half
        q_sw[b, 1] = high_half

    def swap(b, core):
        block = kv.at[core, b]
        return remote(block, block, kv_send, kv_recv.at[b], peer)

    def mine():
        return scal[z // CORES, z % CORES]

    part = tile // HALVES

    def windows(items, start, count):
        rows = slice(start, start + count)
        size = 2 * count
        row = lax.broadcasted_iota(jnp.int32, (size, tile), 0)
        head = row[:, 0:1] < count
        row = jnp.where(row < count, row, row - count) + start
        column = lanes((size, tile))
        causal = column <= row
        own_scal = mine()
        sink = jnp.where(head, own_scal[1:2, 0:1], own_scal[2:3, 0:1])
        pairs = [
            (
                kv[c, i, :, 2 * wide : 4 * wide],
                kv[1 - c, jnp.maximum(i - 1 + c, 0), :, 2 * wide : 4 * wide],
            )
            for i in items
        ]
        scores = []
        for i, (near, far) in zip(items, pairs):
            q = q_sw[i, :, rows, :].reshape(size, wide)
            far_ok = (column > row) & (2 * i + c > 0)
            scores.append(
                (
                    jnp.where(causal, dot_t(q, near[:, 0:wide]), -jnp.inf),
                    jnp.where(far_ok, dot_t(q, far[:, 0:wide]), -jnp.inf),
                )
            )
        tops = [
            jnp.maximum(jnp.max(jnp.maximum(*two), axis=-1, keepdims=True), sink) for two in scores
        ]
        weights_of = [[jnp.exp(one - top) for one in two] for two, top in zip(scores, tops)]
        totals = [
            jnp.sum(two[0] + two[1], axis=-1, keepdims=True) + jnp.exp(sink - top)
            for two, top in zip(weights_of, tops)
        ]
        low_part = lanes((count, wide)) < HD
        for i, (near, far), two, total in zip(items, pairs, weights_of, totals):
            two = [one.astype(BF16) for one in two]
            summed = dot(two[0], near[:, wide : 2 * wide]) + dot(two[1], far[:, wide : 2 * wide])
            result = summed / total
            rows_out[i, 1, rows, :] = jnp.where(low_part, result[0:count], result[count:size]).astype(BF16)

    def spread(i, half):
        rows = slice(half * part, (half + 1) * part)
        size = 2 * part
        q = q_da[i, :, rows, :].reshape(size, wide)
        row = lax.broadcasted_iota(jnp.int32, (size, tile), 0)
        row = jnp.where(row < part, row, row - part) + half * part
        column = lanes((size, tile))
        scores = []
        top = None
        for h in range(2):
            keys = kv[h, 0 : i + 1, :, 0:wide].reshape((i + 1) * tile, wide)
            s = dot_t(q, keys)
            tiles = [s[:, j * tile : (j + 1) * tile] for j in range(i + 1)]
            tiles[i] = jnp.where(column + (h - c) * tile <= row, tiles[i], -jnp.inf)
            scores.append(tiles)
            for one in tiles:
                top = one if top is None else jnp.maximum(top, one)
        top = jnp.max(top, axis=-1, keepdims=True)
        total = None
        summed = None
        for h in range(2):
            weights = [jnp.exp(one - top) for one in scores[h]]
            for one in weights:
                total = one if total is None else total + one
            values = kv[h, 0 : i + 1, :, wide : 2 * wide].reshape((i + 1) * tile, wide)
            flat = jnp.concatenate([one.astype(BF16) for one in weights], axis=-1)
            step = dot(flat, values)
            summed = step if summed is None else summed + step
        total = jnp.sum(total, axis=-1, keepdims=True)
        maps = summed / total
        blend = maps[0:part] - mine()[0:1, :] * maps[part:size]
        return rms_norm(blend, head_gain[...]).astype(BF16)

    def send_rows(i, j, half):
        rows = pl.ds(half * part, part)
        go(
            remote(
                rows_out.at[i, j, rows],
                rows_in.at[j, z, rows],
                r_send,
                r_recv.at[j, half],
                {"sp": i},
            ),
            z != i,
        )

        @pl.when(z == i)
        def _():
            rows = slice(half * part, (half + 1) * part)
            rows_in[j, i, rows, :] = rows_out[i, j, rows, :]

    def await_rows(j, half):
        block = rows_in.at[j, 0 : n - 1, pl.ds(half * part, part)]
        remote(block, block, r_send, r_recv.at[j, half], peer).wait_recv()

    def opening(zz, cc):
        targets = [zt for zt in (CORES * cc, CORES * cc + 1) if zt != zz]
        targets.sort(key=lambda zt: -abs(zt - zz))
        for s in range(CUTS):
            for zt in targets:
                send_weight(zz, zt, s)
        for p in range(PIECES):
            for d in range(2):
                hop(zz, d, 0, p)

    def reach(zz, d):
        return zz if d == 0 else n - 1 - zz

    def steps(*names):
        def script(zz, cc):
            for kind, k, p in names:
                if kind == "W":
                    for far in range(1, n):
                        for d in range(2):
                            if far <= reach(zz, d):
                                event_w(zz - far * way(d), p)
                elif kind == "Y":
                    for far in range(1, n):
                        for d in range(2):
                            if far <= reach(zz, d):
                                event_y(zz - far * way(d), p)
                else:
                    d = cc if kind == "E" else 1 - cc
                    if k <= reach(zz, d):
                        event_x(zz, d, k, p)

        return script

    blocks = (
        z,
        z + 1 - 2 * (z % 2),
        jnp.where(z < 2, 2, 1),
        jnp.where(z < 2, 3, 0),
    )

    own_w = remote(wp.at[z % CORES], wb.at[z], own_send, own_recv, peer)
    own_local = pltpu.make_async_copy(wp.at[z % CORES], wb.at[z], local_sem.at[12])
    sc = remote(scal.at[c], scal.at[c], sc_send, sc_recv, peer)

    def share(j, part):
        rows = wout.shape[2] // SHARES
        block = wout.at[j, c, pl.ds(part * rows, rows)]
        return remote(block, block, wo_send, wo_recv, peer)

    def share_all():
        pltpu.make_async_copy(wout.at[:, c], wout.at[:, c], local_sem.at[11]).wait()
        for j in range(2):
            for part in range(SHARES):
                share(j, part).start()


    run(opening)
    go(own_w, owner)
    pl.when(owner)(own_local.start)
    go(sc)

    run(
        steps(
            ("E", 1, 0),
            ("W", 0, 0),
            ("E", 1, 1),
            ("W", 0, 1),
            ("E", 2, 0),
            ("E", 1, 2),
            ("W", 0, 2),
            ("E", 2, 1),
            ("E", 1, 3),
            ("W", 0, 3),
            ("Y", 0, 0),
            ("E", 2, 2),
            ("L", 1, 0),
            ("E", 2, 3),
            ("L", 1, 1),
            ("Y", 0, 1),
            ("E", 3, 0),
            ("L", 1, 2),
            ("E", 3, 1),
            ("L", 1, 3),
            ("Y", 0, 2),
            ("E", 3, 2),
            ("L", 2, 0),
            ("E", 3, 3),
            ("L", 2, 1),
            ("L", 2, 2),
            ("L", 2, 3),
            ("Y", 0, 3),
        )
    )
    pl.when(owner)(own_local.wait)
    pl.when(jnp.logical_not(owner))(own_w.wait_recv)
    theirs = wb.at[0 : n - 1, :, 1 - c]
    remote(theirs, theirs, wc_send, wc_recv, peer).wait_recv()
    run(
        steps(
            ("L", 3, 0),
        )
    )
    project(blocks[0])
    run(
        steps(
            ("L", 3, 1),
        )
    )
    arrive(blocks[1])
    project(blocks[1])
    run(
        steps(
            ("L", 3, 2),
            ("L", 3, 3),
        )
    )
    arrive(blocks[2])
    project(blocks[2])
    remote(scal.at[1 - c], scal.at[1 - c], sc_send, sc_recv, peer).wait_recv()
    for b in blocks[:3]:
        swap(b, 1 - c).wait_recv()
    windows((jnp.where(z < 2, 1, 3), 2), 0, tile)
    arrive(blocks[3])
    project(blocks[3])
    share_all()
    swap(blocks[3], 1 - c).wait_recv()
    for half in range(HALVES):
        rows = slice(half * part, (half + 1) * part)
        windows((jnp.where(z < 2, 0, 1), jnp.where(z < 2, 3, 0)), half * part, part)
        for i in (3, 0, 2, 1):
            send_rows(i, 1, half)
        for i in (3, 0):
            rows_out[i, 0, rows, :] = spread(i, half)
        for i in (3, 0):
            send_rows(i, 0, half)
        for i in (2, 1):
            rows_out[i, 0, rows, :] = spread(i, half)
        for i in (2, 1):
            send_rows(i, 0, half)

    share_in = wout.at[:, 1 - c]
    remote(share_in, share_in, wo_send, wo_recv, peer).wait_recv()
    columns = out_ref.shape[2] // COLUMNS

    def span(half, q):
        return pl.ds(half * part, part), pl.ds(q * columns, columns)

    def summing(half, q):
        rows, cols = span(half, q)
        return remote(
            sum_out.at[rows, cols],
            sum_in.at[rows, cols],
            s_send,
            s_recv.at[half, q],
            across,
        )

    def finish(half, q):
        rows, cols = span(half, q)
        summing(half, q).wait_recv()
        out_ref[c, rows, cols] = (sum_out[rows, cols].astype(F32) + sum_in[rows, cols].astype(F32)).astype(BF16)
        block = out_ref.at[c, rows, cols]
        go(remote(block, block, o_send, o_recv, peer))

    for half in range(HALVES):
        rows = slice(half * part, (half + 1) * part)
        await_rows(1, half)
        await_rows(0, half)
        for q in range(COLUMNS):
            cols = slice(q * columns, (q + 1) * columns)
            acc = None
            for j in range(2):
                values = jnp.concatenate([rows_in[j, zs, rows, :] for zs in range(n)], axis=-1)
                step = dot(values, wout[j, :, :, cols].reshape(2 * wout.shape[2], columns))
                acc = step if acc is None else acc + step
            sum_out[rows, cols] = acc.astype(BF16)
            go(summing(half, q))
    for half in range(HALVES):
        for q in range(COLUMNS):
            finish(half, q)
    block = out_ref.at[1 - c]
    remote(block, block, o_send, o_recv, peer).wait_recv()

    def drained(ref, sem):
        remote(ref, ref, sem, o_recv, peer).wait_send()

    for zz in range(n):

        @pl.when(z == zz)
        def _(zz=zz):
            if zz + 1 < n:
                drained(xg.at[0 : zz + 1, x], x_send.at[0])
            if zz >= 1:
                drained(xg.at[0 : n - zz, x], x_send.at[1])

    drained(xg.at[0 : n - 1, x], xf_send)
    pl.when(owner)(lambda: drained(wp.at[0, y], w_send))
    pl.when(jnp.logical_not(owner))(lambda: drained(wp.at[:, y], w_send))
    pl.when(owner)(lambda: drained(wp.at[0], own_send))
    drained(wb.at[0 : n - 1, y, c], wy_send)
    drained(wb.at[0 : n - 1, :, c], wc_send)
    drained(scal.at[c], sc_send)
    drained(wout.at[:, c], wo_send)
    drained(kv.at[c], kv_send)
    drained(rows_out.at[0 : n - 1], r_send)
    drained(sum_out, s_send)
    drained(out_ref.at[c], o_send)


def transposed(n, *arrays):
    (
        inputs,
        norm_gain,
        da_query_weight,
        da_key_weight,
        da_value_weight,
        sw_query_weight,
        sw_key_weight,
        sw_value_weight,
        da_query_gain,
        da_key_gain,
        sw_query_gain,
        sw_key_gain,
        mix_lambda,
        head_gain,
        sink_logit,
        da_out_weight,
        sw_out_weight,
    ) = arrays
    rows, d = inputs.shape
    depth = da_query_weight.shape[0]
    wide = 2 * HD
    width = 5 * wide
    cut_rows = depth // 4 // CUTS
    tile = rows // 2
    part = tile // 2 // PIECES
    group = da_out_weight.shape[0]

    def cut(weight):
        return weight.reshape(2, CORES, CUTS, cut_rows, weight.shape[1])

    def line(vector):
        return vector.reshape(1, -1)

    DMA = pltpu.SemaphoreType.DMA
    any_space = pl.BlockSpec(memory_space=pl.ANY)
    out = pl.pallas_call(
        functools.partial(kernel, n),
        out_shape=pltpu.VMEM((2, tile, d), BF16),
        in_specs=[any_space] * 17,
        out_specs=pl.BlockSpec(memory_space=pltpu.VMEM),
        scratch_shapes=[
            pltpu.VMEM((2, PIECES, part, d), BF16),
            pltpu.VMEM((2, 2, CORES, CUTS, cut_rows, wide), BF16),
            pltpu.VMEM((1, d), F32),
            pltpu.VMEM((1, HD), F32),
            pltpu.VMEM((1, HD), F32),
            pltpu.VMEM((1, HD), F32),
            pltpu.VMEM((1, HD), F32),
            pltpu.VMEM((1, wide), F32),
            pltpu.VMEM((1, mix_lambda.shape[0]), F32),
            pltpu.VMEM((1, sink_logit.shape[0]), F32),
            pltpu.VMEM((2, CORES, group, d), BF16),
            pltpu.VMEM((CORES, 2, CORES, CUTS, cut_rows, width), BF16),
            pltpu.VMEM((n, 2, PIECES, part, d), BF16),
            pltpu.VMEM((n, 2, CORES, CUTS, cut_rows, width), BF16),
            pltpu.VMEM((n, 2, tile, wide), BF16),
            pltpu.VMEM((n, 2, tile, wide), BF16),
            pltpu.VMEM((CORES, n, tile, 4 * wide), BF16),
            pltpu.VMEM((CORES, CORES, 8, wide), F32),
            pltpu.VMEM((n, 2, tile, wide), BF16),
            pltpu.VMEM((2, n, tile, wide), BF16),
            pltpu.VMEM((tile, d), BF16),
            pltpu.VMEM((tile, d), BF16),
            DMA((14,)),
            DMA((2,)),
            DMA((2, n - 1, PIECES)),
            DMA,
            DMA((n,)),
            DMA,
            DMA((n, CUTS)),
            DMA,
            DMA((n, CUTS)),
            DMA,
            DMA,
            DMA,
            DMA,
            DMA,
            DMA((n,)),
            DMA,
            DMA,
            DMA,
            DMA,
            DMA,
            DMA((2, HALVES)),
            DMA,
            DMA((HALVES, COLUMNS)),
            DMA,
            DMA,
        ],
        compiler_params=pltpu.CompilerParams(
            collective_id=0, has_side_effects=True, vmem_limit_bytes=60 * 1024 * 1024
        ),
    )(
        inputs.reshape(CORES, 2, PIECES, part, d),
        cut(da_query_weight),
        cut(da_key_weight),
        cut(da_value_weight),
        cut(sw_query_weight),
        cut(sw_key_weight),
        cut(sw_value_weight),
        line(norm_gain),
        line(da_query_gain),
        line(da_key_gain),
        line(sw_query_gain),
        line(sw_key_gain),
        line(head_gain),
        line(mix_lambda),
        line(sink_logit),
        da_out_weight,
        sw_out_weight,
    )
    return out.reshape(rows, d)


def body(sizes, *arrays):
    rows = arrays[0].shape[0]
    heads = arrays[12].shape[0]
    sinks = arrays[14].shape[0]
    n = sizes["sp"]
    fits = (
        sizes["grp"] == 2
        and sizes["tp"] == 2 * CORES
        and n == 2 * CORES
        and heads == CORES
        and sinks == 2 * CORES
        and arrays[6].shape[1] == CORES * HD
        and rows == 2 * WINDOW
    )
    if fits:
        return transposed(n, *arrays)
    return on_device(*arrays)


def solution(mesh):
    return jax.shard_map(
        functools.partial(body, dict(mesh.shape)),
        mesh=mesh,
        in_specs=(
            P(("grp", "sp"), None),
            P(),
            P("sp", "tp"),
            P("sp", "tp"),
            P("sp", "tp"),
            P("sp", "tp"),
            P("sp", "tp"),
            P("sp", "tp"),
            P(),
            P(),
            P(),
            P(),
            P("tp"),
            P(),
            P("tp"),
            P("tp", None),
            P("tp", None),
        ),
        out_specs=P(("grp", "sp"), None),
        check_vma=False,
    )
```

```python
import functools

import jax
import jax.numpy as jnp
from jax import lax
from jax.experimental import pallas as pl
from jax.experimental.pallas import tpu as pltpu
from jax.sharding import PartitionSpec as P

HD = 64
WINDOW = 128


def shifted(value, axis, steps):
    count = lax.axis_size(axis)
    first, last = (max(0, -steps), min(count, count - steps))
    return lax.ppermute(value, axis, [(source, source + steps) for source in range(first, last)])


def rms_norm(values, gain):
    return values * lax.rsqrt(jnp.mean(values * values, axis=-1, keepdims=True) + 1e-06) * gain


def absorb(state, queries, places, keys, values, key_places):
    top, total, summed = state
    scores = jnp.einsum(
        "qhmd,khmd->hmqk", queries, keys, preferred_element_type=jnp.float32
    ) * HD ** (-0.5)
    scores = jnp.where(key_places[None, :] <= places[:, None], scores, -jnp.inf)
    new_top = jnp.maximum(top, jnp.max(scores, axis=-1))
    weights = jnp.exp(scores - new_top[..., None])
    total = jnp.sum(weights, axis=-1)
    summed = jnp.einsum(
        "hmqk,khe->hmqe", weights.astype(jnp.bfloat16), values, preferred_element_type=jnp.float32
    )
    return (new_top, total, summed)


def keep(state, queries, places, keys, values, key_places):
    return state


def diff_attention(queries, places, da_key, da_value, mix_lambda, head_gain):
    rows = queries.shape[0]
    heads = queries.shape[1]
    half = rows // 2
    fresh = (
        jnp.full((heads, 2, half), -1e30, jnp.float32),
        jnp.zeros((heads, 2, half), jnp.float32),
        jnp.zeros((heads, 2, half, 2 * HD), jnp.float32),
    )
    states = (fresh, fresh)
    start = jnp.int32(0)
    keys = lax.all_gather(da_key, "sp", axis=0, tiled=True)
    values = lax.all_gather(da_value, "sp", axis=0, tiled=True)
    key_places = jnp.arange(keys.shape[0], dtype=jnp.int32)
    updated = []
    for section in range(2):
        own_rows = queries[section * half : (section + 1) * half]
        own_places = places[section * half : (section + 1) * half]
        updated.append(
            lax.cond(
                start <= jnp.max(own_places),
                absorb,
                keep,
                states[section],
                own_rows,
                own_places,
                keys,
                values,
                key_places,
            )
        )
    states = tuple(updated)
    blended = []
    for top, total, summed in states:
        maps = summed / total[..., None]
        blended.append(maps[:, 0] - mix_lambda[:, None, None] * maps[:, 1])
    blend = jnp.transpose(jnp.concatenate(blended, axis=1), (1, 0, 2))
    return rms_norm(blend, head_gain).astype(jnp.bfloat16).reshape(rows, heads * 2 * HD)


def window_attention(sw_query, sw_key, sw_value, earlier_key, earlier_value, sink_logit, first):
    rows = sw_query.shape[0]
    sw_heads = sw_query.shape[1]
    kv_heads = sw_key.shape[1]
    groups = sw_heads // kv_heads
    count = rows // WINDOW

    def band(own, earlier_tile):
        tiles = own.reshape(count, WINDOW, kv_heads, HD)
        earlier = jnp.concatenate([earlier_tile[None], tiles[:-1]], axis=0)
        return jnp.concatenate([earlier, tiles], axis=1)

    key_band = band(sw_key, earlier_key)
    value_band = band(sw_value, earlier_value)
    query_tiles = sw_query.reshape(count, WINDOW, kv_heads, groups, HD)
    scores = jnp.einsum(
        "nqhgd,nkhd->nhgqk", query_tiles, key_band, preferred_element_type=jnp.float32
    ) * HD ** (-0.5)
    lag = WINDOW + jnp.arange(WINDOW)[:, None] - jnp.arange(2 * WINDOW)[None, :]
    key_places = (
        first + jnp.arange(count)[:, None] * WINDOW - WINDOW + jnp.arange(2 * WINDOW)[None, :]
    )
    valid = ((lag >= 0) & (lag < WINDOW))[None] & (key_places >= 0)[:, None, :]
    scores = jnp.where(valid[:, None, None], scores, -jnp.inf)
    sink = sink_logit.reshape(kv_heads, groups)[None, :, :, None]
    top = jnp.maximum(jnp.max(scores, axis=-1), sink)
    weights = jnp.exp(scores - top[..., None])
    total = jnp.sum(weights, axis=-1) + jnp.exp(sink - top)
    summed = jnp.einsum(
        "nhgqk,nkhd->nqhgd",
        weights.astype(jnp.bfloat16),
        value_band,
        preferred_element_type=jnp.float32,
    )
    return (
        (summed / jnp.transpose(total, (0, 3, 1, 2))[..., None])
        .astype(jnp.bfloat16)
        .reshape(rows, sw_heads * HD)
    )


def on_device(
    inputs,
    norm_gain,
    da_query_weight,
    da_key_weight,
    da_value_weight,
    sw_query_weight,
    sw_key_weight,
    sw_value_weight,
    da_query_gain,
    da_key_gain,
    sw_query_gain,
    sw_key_gain,
    mix_lambda,
    head_gain,
    sink_logit,
    da_out_weight,
    sw_out_weight,
):
    rows = inputs.shape[0]
    normed = rms_norm(inputs.astype(jnp.float32), norm_gain).astype(jnp.bfloat16)
    pieces = (
        lax.all_gather(da_query_weight, "sp", axis=0, tiled=True),
        lax.all_gather(da_key_weight, "sp", axis=0, tiled=True),
        lax.all_gather(da_value_weight, "sp", axis=0, tiled=True),
        lax.all_gather(sw_query_weight, "sp", axis=0, tiled=True),
        lax.all_gather(sw_key_weight, "sp", axis=0, tiled=True),
        lax.all_gather(sw_value_weight, "sp", axis=0, tiled=True),
    )
    projected = tuple(
        (jnp.dot(normed, piece, preferred_element_type=jnp.float32) for piece in pieces)
    )
    da_heads = da_query_weight.shape[1] // (2 * HD)
    sw_heads = sw_query_weight.shape[1] // HD
    kv_heads = sw_key_weight.shape[1] // HD
    da_query = rms_norm(projected[0].reshape(rows, da_heads, 2, HD), da_query_gain).astype(
        jnp.bfloat16
    )
    da_key = rms_norm(projected[1].reshape(rows, da_heads, 2, HD), da_key_gain).astype(jnp.bfloat16)
    da_value = projected[2].astype(jnp.bfloat16).reshape(rows, da_heads, 2 * HD)
    sw_query = rms_norm(projected[3].reshape(rows, sw_heads, HD), sw_query_gain).astype(
        jnp.bfloat16
    )
    sw_key = rms_norm(projected[4].reshape(rows, kv_heads, HD), sw_key_gain).astype(jnp.bfloat16)
    sw_value = projected[5].astype(jnp.bfloat16).reshape(rows, kv_heads, HD)
    place = lax.axis_index("sp")
    first = place * rows
    earlier_key, earlier_value = shifted(
        (sw_key[rows - WINDOW :], sw_value[rows - WINDOW :]), "sp", 1
    )
    sw_rows = window_attention(
        sw_query, sw_key, sw_value, earlier_key, earlier_value, sink_logit, first
    )
    places = first + jnp.arange(rows, dtype=jnp.int32)
    da_rows = diff_attention(da_query, places, da_key, da_value, mix_lambda, head_gain)
    partial_value = jnp.dot(da_rows, da_out_weight, preferred_element_type=jnp.float32) + jnp.dot(
        sw_rows, sw_out_weight, preferred_element_type=jnp.float32
    )
    return lax.psum(partial_value.astype(jnp.bfloat16), "tp")


MESH = pl.DeviceIdType.MESH
F32, BF16 = jnp.float32, jnp.bfloat16
CORES = 2


def dot(a, b):
    return jnp.dot(a, b, preferred_element_type=F32)


def dot_t(a, b):
    return lax.dot_general(a, b, (((1,), (1,)), ((), ())), preferred_element_type=F32)


def pair_norm(values, gain):
    lane = lax.broadcasted_iota(jnp.int32, values.shape, 1)
    squares = values * values
    low = jnp.sum(jnp.where(lane < HD, squares, 0.0), axis=-1, keepdims=True)
    high = jnp.sum(jnp.where(lane < HD, 0.0, squares), axis=-1, keepdims=True)
    mean = jnp.where(lane < HD, low, high) * (1.0 / HD)
    return values * lax.rsqrt(mean + 1e-06) * gain


PIECES = 4
CUTS = 4
EIGHTHS = (0, 3, 8)
HALVES = len(EIGHTHS) - 1
COLUMNS = 4
SHARES = 4


def kernel(
    n,
    x_hbm,
    da_q_hbm,
    da_k_hbm,
    da_v_hbm,
    sw_q_hbm,
    sw_k_hbm,
    sw_v_hbm,
    norm_gain_hbm,
    da_q_gain_hbm,
    da_k_gain_hbm,
    sw_q_gain_hbm,
    sw_k_gain_hbm,
    head_gain_hbm,
    mix_hbm,
    sink_hbm,
    da_out_hbm,
    sw_out_hbm,
    out_ref,
    x_raw,
    skv_raw,
    norm_gain,
    da_q_gain,
    da_k_gain,
    sw_q_gain,
    sw_k_gain,
    head_gain,
    mix_ref,
    sink_ref,
    wout,
    wp,
    xg,
    wb,
    q_da,
    q_sw,
    kv,
    scal,
    rows_out,
    rows_in,
    sum_out,
    sum_in,
    local_sem,
    x_send,
    x_recv,
    xf_send,
    xf_recv,
    w_send,
    w_recv,
    wy_send,
    wy_recv,
    wc_send,
    wc_recv,
    own_send,
    own_recv,
    kv_send,
    kv_recv,
    sc_send,
    sc_recv,
    wo_send,
    wo_recv,
    r_send,
    r_recv,
    s_send,
    s_recv,
    o_send,
    o_recv,
):
    y = lax.axis_index("grp")
    z = lax.axis_index("sp")
    t = lax.axis_index("tp")
    x = t // CORES
    c = t % CORES
    peer = {"tp": x * CORES + 1 - c}
    across = {"tp": (1 - x) * CORES + c}
    beside = {"grp": 1 - y}
    wide = 2 * HD

    def at(zz, cc):
        return {"sp": zz, "tp": x * CORES + cc}

    def remote(src, dst, send, recv, device):
        return pltpu.make_async_remote_copy(
            src_ref=src,
            dst_ref=dst,
            send_sem=send,
            recv_sem=recv,
            device_id=device,
            device_id_type=MESH,
        )

    def go(copy, when=None):
        if when is None:
            copy.start()
        else:
            pl.when(when)(copy.start)

    barrier = pltpu.get_barrier_semaphore()

    def greet(device):
        pl.semaphore_signal(barrier, inc=1, device_id=device, device_id_type=MESH)

    for k in range(n - 1, 0, -1):
        for cc in range(CORES):
            greet(at(lax.rem(z + k, n), cc))
    greet(across)
    greet(beside)
    greet(peer)

    load_x = pltpu.make_async_copy(x_hbm.at[c], x_raw, local_sem.at[0])
    load_x.start()
    smalls = []
    for i, (source, target) in enumerate(
        (
            (norm_gain_hbm, norm_gain),
            (da_q_gain_hbm, da_q_gain),
            (da_k_gain_hbm, da_k_gain),
            (sw_q_gain_hbm, sw_q_gain),
            (sw_k_gain_hbm, sw_k_gain),
            (head_gain_hbm, head_gain),
            (mix_hbm, mix_ref),
            (sink_hbm, sink_ref),
        )
    ):
        smalls.append(pltpu.make_async_copy(source, target, local_sem.at[1 + i]))
        smalls[-1].start()
    for j, source in enumerate((sw_k_hbm, sw_v_hbm)):
        pltpu.make_async_copy(source, skv_raw.at[j], local_sem.at[9]).start()
    for par in range(CORES):
        for j, source in enumerate((da_q_hbm, da_k_hbm, da_v_hbm, sw_q_hbm)):
            pltpu.make_async_copy(
                source.at[:, :, :, :, pl.ds(par * wide, wide)],
                wp.at[par, :, :, :, :, pl.ds(j * wide, wide)],
                local_sem.at[10],
            ).start()
    for j, source in enumerate((da_out_hbm, sw_out_hbm)):
        pltpu.make_async_copy(source, wout.at[j, c], local_sem.at[11]).start()

    smalls[0].wait()
    load_x.wait()
    for h in range(2):
        for p in range(PIECES):
            values = rms_norm(x_raw[h, p].astype(F32), norm_gain[...])
            xg[z, h, p] = values.astype(BF16)
    pltpu.make_async_copy(skv_raw, skv_raw, local_sem.at[9]).wait()
    for par in range(CORES):
        cols = slice(par * HD, (par + 1) * HD)
        wp[par, :, :, :, :, 4 * wide : 5 * wide] = jnp.concatenate(
            [skv_raw[0, ..., cols], skv_raw[1, ..., cols]], axis=-1
        )
    for load in smalls[1:]:
        load.wait()
    for par in range(CORES):
        scal[c, par, 0:1, :] = jnp.broadcast_to(mix_ref[:, par : par + 1], (1, wide))
        for g in range(2):
            sink = sink_ref[:, 2 * par + g : 2 * par + g + 1]
            scal[c, par, 1 + g : 2 + g, :] = jnp.broadcast_to(sink, (1, wide))
    packed = wp.at[:, :, :, :, :, pl.ds(0, 4 * wide)]
    pltpu.make_async_copy(packed, packed, local_sem.at[10]).wait()
    pl.semaphore_wait(barrier, 3 + (n - 1) * CORES)

    def way(d):
        return 1 - 2 * d

    def cross(zs, p):
        piece = xg.at[zs, x, p]
        return remote(piece, piece, xf_send, xf_recv.at[zs], across)

    owner = c == z // CORES

    def hop(zz, d, k, p):
        source, target = zz - k * way(d), zz + way(d)
        if 0 <= target < n:
            piece = xg.at[source, x, p]
            remote(piece, piece, x_send.at[d], x_recv.at[d, k, p], {"sp": target}).start()

    def weight_beside(zs, yy, s):
        piece = wb.at[zs, yy, c, s]
        return remote(piece, piece, wy_send, wy_recv.at[zs, s], beside)

    def weight_core(zs, yy, s):
        piece = wb.at[zs, yy, c, s]
        return remote(piece, piece, wc_send, wc_recv, peer)

    def event_x(zz, d, k, p):
        zs = zz - k * way(d)
        piece = xg.at[zs, x, p]
        remote(piece, piece, x_send.at[d], x_recv.at[d, k - 1, p], across).wait_recv()
        if k < n - 1:
            hop(zz, d, k, p)
        cross(zs, p).start()

    def event_w(zs, s):
        piece = wb.at[zs, y, c, s]
        remote(piece, piece, w_send, w_recv.at[zs, s], peer).wait_recv()
        weight_beside(zs, y, s).start()
        weight_core(zs, y, s).start()

    def event_y(zs, s):
        weight_beside(zs, 1 - y, s).wait_recv()
        weight_core(zs, 1 - y, s).start()

    def send_weight(zz, zt, s):
        for cd in range(CORES):
            remote(
                wp.at[zt % CORES, y, cd, s],
                wb.at[zz, y, cd, s],
                w_send,
                w_recv.at[zz, s],
                at(zt, cd),
            ).start()

    def run(script):
        for zz in range(n):
            for cc in range(CORES):

                @pl.when((z == zz) & (c == cc))
                def _(zz=zz, cc=cc):
                    script(zz, cc)

    tile = xg.shape[1] * xg.shape[2] * xg.shape[3]
    depth = wb.shape[1] * wb.shape[2] * wb.shape[3] * wb.shape[4]
    width = wb.shape[5]

    def lanes(shape):
        return lax.broadcasted_iota(jnp.int32, shape, len(shape) - 1)

    low = lanes((tile, wide)) < HD

    def twice(ref):
        return jnp.concatenate([ref[...], ref[...]], axis=-1)

    normed = pair_norm

    def arrive(b):
        @pl.when(b != z)
        def _():
            block = xg.at[b, 1 - x]
            remote(block, block, xf_send, xf_recv.at[b], across).wait_recv()

    def project(b):
        block = xg[b].reshape(tile, xg.shape[4])
        acc = dot(block[:, 0:depth], wb[0].reshape(depth, width))
        for j in range(1, n):
            acc += dot(block[:, j * depth : (j + 1) * depth], wb[j].reshape(depth, width))
        scale = HD ** (-0.5)

        def heads(values, gain):
            result = normed(values, gain).astype(BF16).astype(F32) * scale
            low_half = jnp.where(low, result, 0.0).astype(BF16)
            high_half = jnp.where(low, 0.0, result).astype(BF16)
            return low_half, high_half

        key = normed(acc[:, wide : 2 * wide], twice(da_k_gain))
        kv[c, b, :, 0:wide] = key.astype(BF16)
        kv[c, b, :, wide : 2 * wide] = acc[:, 2 * wide : 3 * wide].astype(BF16)
        pair = acc[:, 4 * wide : 5 * wide]
        pair = jnp.where(low, normed(pair, twice(sw_k_gain)), pair).astype(BF16)
        row = lax.broadcasted_iota(jnp.int32, (wide, 2 * wide), 0)
        column = lanes((wide, 2 * wide))
        source = column % HD + jnp.where(column < wide, 0, HD)
        doubler = jnp.where(row == source, 1.0, 0.0).astype(BF16)
        kv[c, b, :, 2 * wide : 4 * wide] = dot(pair, doubler).astype(BF16)
        swap(b, c).start()
        low_half, high_half = heads(acc[:, 0:wide], twice(da_q_gain))
        q_da[b, 0] = low_half
        q_da[b, 1] = high_half
        low_half, high_half = heads(acc[:, 3 * wide : 4 * wide], twice(sw_q_gain))
        q_sw[b, 0] = low_half
        q_sw[b, 1] = high_half

    def swap(b, core):
        block = kv.at[core, b]
        return remote(block, block, kv_send, kv_recv.at[b], peer)

    def mine():
        return scal[z // CORES, z % CORES]

    bounds = [tile * e // 8 for e in EIGHTHS]

    def rows_of(half):
        return bounds[half], bounds[half + 1] - bounds[half]

    def windows(items, start, count):
        rows = slice(start, start + count)
        size = 2 * count
        row = lax.broadcasted_iota(jnp.int32, (size, tile), 0)
        head = row[:, 0:1] < count
        row = jnp.where(row < count, row, row - count) + start
        column = lanes((size, tile))
        causal = column <= row
        own_scal = mine()
        sink = jnp.where(head, own_scal[1:2, 0:1], own_scal[2:3, 0:1])
        pairs = [
            (
                kv[c, i, :, 2 * wide : 4 * wide],
                kv[1 - c, jnp.maximum(i - 1 + c, 0), :, 2 * wide : 4 * wide],
            )
            for i in items
        ]
        scores = []
        for i, (near, far) in zip(items, pairs):
            q = q_sw[i, :, rows, :].reshape(size, wide)
            far_ok = (column > row) & (2 * i + c > 0)
            scores.append(
                (
                    jnp.where(causal, dot_t(q, near[:, 0:wide]), -jnp.inf),
                    jnp.where(far_ok, dot_t(q, far[:, 0:wide]), -jnp.inf),
                )
            )
        tops = [
            jnp.maximum(jnp.max(jnp.maximum(*two), axis=-1, keepdims=True), sink) for two in scores
        ]
        weights_of = [[jnp.exp(one - top) for one in two] for two, top in zip(scores, tops)]
        totals = [
            jnp.sum(two[0] + two[1], axis=-1, keepdims=True) + jnp.exp(sink - top)
            for two, top in zip(weights_of, tops)
        ]
        low_part = lanes((count, wide)) < HD
        for i, (near, far), two, total in zip(items, pairs, weights_of, totals):
            two = [one.astype(BF16) for one in two]
            summed = dot(two[0], near[:, wide : 2 * wide]) + dot(two[1], far[:, wide : 2 * wide])
            result = summed / total
            rows_out[i, 1, rows, :] = jnp.where(low_part, result[0:count], result[count:size]).astype(BF16)

    def spread(i, half):
        start, part = rows_of(half)
        rows = slice(start, start + part)
        size = 2 * part
        q = q_da[i, :, rows, :].reshape(size, wide)
        row = lax.broadcasted_iota(jnp.int32, (size, tile), 0)
        row = jnp.where(row < part, row, row - part) + start
        column = lanes((size, tile))
        scores = []
        top = None
        for h in range(2):
            keys = kv[h, 0 : i + 1, :, 0:wide].reshape((i + 1) * tile, wide)
            s = dot_t(q, keys)
            tiles = [s[:, j * tile : (j + 1) * tile] for j in range(i + 1)]
            tiles[i] = jnp.where(column + (h - c) * tile <= row, tiles[i], -jnp.inf)
            scores.append(tiles)
            for one in tiles:
                top = one if top is None else jnp.maximum(top, one)
        top = jnp.max(top, axis=-1, keepdims=True)
        total = None
        summed = None
        for h in range(2):
            weights = [jnp.exp(one - top) for one in scores[h]]
            for one in weights:
                total = one if total is None else total + one
            values = kv[h, 0 : i + 1, :, wide : 2 * wide].reshape((i + 1) * tile, wide)
            flat = jnp.concatenate([one.astype(BF16) for one in weights], axis=-1)
            step = dot(flat, values)
            summed = step if summed is None else summed + step
        total = jnp.sum(total, axis=-1, keepdims=True)
        maps = summed / total
        blend = maps[0:part] - mine()[0:1, :] * maps[part:size]
        return rms_norm(blend, head_gain[...]).astype(BF16)

    def send_rows(i, j, half):
        rows = pl.ds(*rows_of(half))
        go(
            remote(
                rows_out.at[i, j, rows],
                rows_in.at[j, z, rows],
                r_send,
                r_recv.at[j, half],
                {"sp": i},
            ),
            z != i,
        )

        @pl.when(z == i)
        def _():
            rows = slice(bounds[half], bounds[half + 1])
            rows_in[j, i, rows, :] = rows_out[i, j, rows, :]

    def await_rows(j, half):
        block = rows_in.at[j, 0 : n - 1, pl.ds(*rows_of(half))]
        remote(block, block, r_send, r_recv.at[j, half], peer).wait_recv()

    def opening(zz, cc):
        targets = [zt for zt in (CORES * cc, CORES * cc + 1) if zt != zz]
        targets.sort(key=lambda zt: -abs(zt - zz))
        for s in range(CUTS):
            for zt in targets:
                send_weight(zz, zt, s)
        for p in range(PIECES):
            for d in range(2):
                hop(zz, d, 0, p)

    def reach(zz, d):
        return zz if d == 0 else n - 1 - zz

    def steps(ends, mids):
        def script(zz, cc):
            for kind, k, p in ends if zz in (0, n - 1) else mids:
                if kind == "W":
                    for far in range(1, n):
                        for d in range(2):
                            if far <= reach(zz, d):
                                event_w(zz - far * way(d), p)
                elif kind == "Y":
                    for far in range(1, n):
                        for d in range(2):
                            if far <= reach(zz, d):
                                event_y(zz - far * way(d), p)
                else:
                    d = cc if kind == "E" else 1 - cc
                    if k <= reach(zz, d):
                        event_x(zz, d, k, p)

        return script

    blocks = (
        z,
        z + 1 - 2 * (z % 2),
        jnp.where(z < 2, 2, 1),
        jnp.where(z < 2, 3, 0),
    )

    own_w = remote(wp.at[z % CORES], wb.at[z], own_send, own_recv, peer)
    own_local = pltpu.make_async_copy(wp.at[z % CORES], wb.at[z], local_sem.at[12])
    sc = remote(scal.at[c], scal.at[c], sc_send, sc_recv, peer)

    def share(j, part):
        rows = wout.shape[2] // SHARES
        block = wout.at[j, c, pl.ds(part * rows, rows)]
        return remote(block, block, wo_send, wo_recv, peer)

    def share_all():
        pltpu.make_async_copy(wout.at[:, c], wout.at[:, c], local_sem.at[11]).wait()
        for j in range(2):
            for part in range(SHARES):
                share(j, part).start()


    run(opening)
    go(own_w, owner)
    pl.when(owner)(own_local.start)
    go(sc)

    run(steps((("E", 1, 0), ("W", 0, 0), ("E", 1, 1), ("W", 0, 1), ("E", 1, 2), ("E", 2, 0), ("E", 1, 3), ("E", 2, 1), ("W", 0, 2), ("L", 1, 0), ("E", 2, 2), ("L", 1, 1), ("W", 0, 3), ("L", 1, 2), ("Y", 0, 0), ("E", 2, 3), ("L", 1, 3), ("Y", 0, 1), ("E", 3, 0), ("E", 3, 1), ("Y", 0, 2), ("E", 3, 2), ("L", 2, 0), ("E", 3, 3), ("L", 2, 1), ("L", 2, 2), ("L", 2, 3), ("Y", 0, 3)), (("E", 1, 0), ("W", 0, 0), ("E", 1, 1), ("W", 0, 1), ("E", 1, 2), ("E", 1, 3), ("W", 0, 2), ("E", 2, 0), ("E", 2, 1), ("W", 0, 3), ("L", 1, 0), ("E", 2, 2), ("L", 1, 1), ("E", 2, 3), ("L", 1, 2), ("Y", 0, 0), ("L", 1, 3), ("Y", 0, 1), ("L", 2, 0), ("Y", 0, 2), ("L", 2, 1), ("L", 2, 2), ("L", 2, 3), ("Y", 0, 3))))
    pl.when(owner)(own_local.wait)
    pl.when(jnp.logical_not(owner))(own_w.wait_recv)
    theirs = wb.at[0 : n - 1, :, 1 - c]
    remote(theirs, theirs, wc_send, wc_recv, peer).wait_recv()
    run(steps((("L", 3, 0),), ()))
    project(blocks[0])
    run(steps((("L", 3, 1),), ()))
    arrive(blocks[1])
    project(blocks[1])
    run(steps((("L", 3, 2), ("L", 3, 3)), ()))
    arrive(blocks[2])
    project(blocks[2])
    remote(scal.at[1 - c], scal.at[1 - c], sc_send, sc_recv, peer).wait_recv()
    for b in blocks[:3]:
        swap(b, 1 - c).wait_recv()
    windows((jnp.where(z < 2, 1, 3), 2), 0, tile)
    arrive(blocks[3])
    project(blocks[3])
    share_all()
    swap(blocks[3], 1 - c).wait_recv()
    for half in range(HALVES):
        rows = slice(bounds[half], bounds[half + 1])
        windows((jnp.where(z < 2, 0, 1), jnp.where(z < 2, 3, 0)), *rows_of(half))
        for i in (3, 0, 2, 1):
            send_rows(i, 1, half)
        for i in (3, 0):
            rows_out[i, 0, rows, :] = spread(i, half)
        for i in (3, 0):
            send_rows(i, 0, half)
        for i in (2, 1):
            rows_out[i, 0, rows, :] = spread(i, half)
        for i in (2, 1):
            send_rows(i, 0, half)

    share_in = wout.at[:, 1 - c]
    remote(share_in, share_in, wo_send, wo_recv, peer).wait_recv()
    columns = out_ref.shape[2] // COLUMNS

    def span(half, q):
        return pl.ds(*rows_of(half)), pl.ds(q * columns, columns)

    def summing(half, q):
        rows, cols = span(half, q)
        return remote(
            sum_out.at[rows, cols],
            sum_in.at[rows, cols],
            s_send,
            s_recv.at[half, q],
            across,
        )

    def finish(half, q):
        rows, cols = span(half, q)
        summing(half, q).wait_recv()
        out_ref[c, rows, cols] = (sum_out[rows, cols].astype(F32) + sum_in[rows, cols].astype(F32)).astype(BF16)
        block = out_ref.at[c, rows, cols]
        go(remote(block, block, o_send, o_recv, peer))

    for half in range(HALVES):
        rows = slice(bounds[half], bounds[half + 1])
        await_rows(1, half)
        await_rows(0, half)
        for q in range(COLUMNS):
            cols = slice(q * columns, (q + 1) * columns)
            acc = None
            for j in range(2):
                values = jnp.concatenate([rows_in[j, zs, rows, :] for zs in range(n)], axis=-1)
                step = dot(values, wout[j, :, :, cols].reshape(2 * wout.shape[2], columns))
                acc = step if acc is None else acc + step
            sum_out[rows, cols] = acc.astype(BF16)
            go(summing(half, q))
    for half in range(HALVES):
        for q in range(COLUMNS):
            finish(half, q)
    block = out_ref.at[1 - c]
    remote(block, block, o_send, o_recv, peer).wait_recv()

    def drained(ref, sem):
        remote(ref, ref, sem, o_recv, peer).wait_send()

    for zz in range(n):

        @pl.when(z == zz)
        def _(zz=zz):
            if zz + 1 < n:
                drained(xg.at[0 : zz + 1, x], x_send.at[0])
            if zz >= 1:
                drained(xg.at[0 : n - zz, x], x_send.at[1])

    drained(xg.at[0 : n - 1, x], xf_send)
    pl.when(owner)(lambda: drained(wp.at[0, y], w_send))
    pl.when(jnp.logical_not(owner))(lambda: drained(wp.at[:, y], w_send))
    pl.when(owner)(lambda: drained(wp.at[0], own_send))
    drained(wb.at[0 : n - 1, y, c], wy_send)
    drained(wb.at[0 : n - 1, :, c], wc_send)
    drained(scal.at[c], sc_send)
    drained(wout.at[:, c], wo_send)
    drained(kv.at[c], kv_send)
    drained(rows_out.at[0 : n - 1], r_send)
    drained(sum_out, s_send)
    drained(out_ref.at[c], o_send)


def transposed(n, *arrays):
    (
        inputs,
        norm_gain,
        da_query_weight,
        da_key_weight,
        da_value_weight,
        sw_query_weight,
        sw_key_weight,
        sw_value_weight,
        da_query_gain,
        da_key_gain,
        sw_query_gain,
        sw_key_gain,
        mix_lambda,
        head_gain,
        sink_logit,
        da_out_weight,
        sw_out_weight,
    ) = arrays
    rows, d = inputs.shape
    depth = da_query_weight.shape[0]
    wide = 2 * HD
    width = 5 * wide
    cut_rows = depth // 4 // CUTS
    tile = rows // 2
    part = tile // 2 // PIECES
    group = da_out_weight.shape[0]

    def cut(weight):
        return weight.reshape(2, CORES, CUTS, cut_rows, weight.shape[1])

    def line(vector):
        return vector.reshape(1, -1)

    DMA = pltpu.SemaphoreType.DMA
    any_space = pl.BlockSpec(memory_space=pl.ANY)
    out = pl.pallas_call(
        functools.partial(kernel, n),
        out_shape=pltpu.VMEM((2, tile, d), BF16),
        in_specs=[any_space] * 17,
        out_specs=pl.BlockSpec(memory_space=pltpu.VMEM),
        scratch_shapes=[
            pltpu.VMEM((2, PIECES, part, d), BF16),
            pltpu.VMEM((2, 2, CORES, CUTS, cut_rows, wide), BF16),
            pltpu.VMEM((1, d), F32),
            pltpu.VMEM((1, HD), F32),
            pltpu.VMEM((1, HD), F32),
            pltpu.VMEM((1, HD), F32),
            pltpu.VMEM((1, HD), F32),
            pltpu.VMEM((1, wide), F32),
            pltpu.VMEM((1, mix_lambda.shape[0]), F32),
            pltpu.VMEM((1, sink_logit.shape[0]), F32),
            pltpu.VMEM((2, CORES, group, d), BF16),
            pltpu.VMEM((CORES, 2, CORES, CUTS, cut_rows, width), BF16),
            pltpu.VMEM((n, 2, PIECES, part, d), BF16),
            pltpu.VMEM((n, 2, CORES, CUTS, cut_rows, width), BF16),
            pltpu.VMEM((n, 2, tile, wide), BF16),
            pltpu.VMEM((n, 2, tile, wide), BF16),
            pltpu.VMEM((CORES, n, tile, 4 * wide), BF16),
            pltpu.VMEM((CORES, CORES, 8, wide), F32),
            pltpu.VMEM((n, 2, tile, wide), BF16),
            pltpu.VMEM((2, n, tile, wide), BF16),
            pltpu.VMEM((tile, d), BF16),
            pltpu.VMEM((tile, d), BF16),
            DMA((14,)),
            DMA((2,)),
            DMA((2, n - 1, PIECES)),
            DMA,
            DMA((n,)),
            DMA,
            DMA((n, CUTS)),
            DMA,
            DMA((n, CUTS)),
            DMA,
            DMA,
            DMA,
            DMA,
            DMA,
            DMA((n,)),
            DMA,
            DMA,
            DMA,
            DMA,
            DMA,
            DMA((2, HALVES)),
            DMA,
            DMA((HALVES, COLUMNS)),
            DMA,
            DMA,
        ],
        compiler_params=pltpu.CompilerParams(
            collective_id=0, has_side_effects=True, vmem_limit_bytes=60 * 1024 * 1024
        ),
    )(
        inputs.reshape(CORES, 2, PIECES, part, d),
        cut(da_query_weight),
        cut(da_key_weight),
        cut(da_value_weight),
        cut(sw_query_weight),
        cut(sw_key_weight),
        cut(sw_value_weight),
        line(norm_gain),
        line(da_query_gain),
        line(da_key_gain),
        line(sw_query_gain),
        line(sw_key_gain),
        line(head_gain),
        line(mix_lambda),
        line(sink_logit),
        da_out_weight,
        sw_out_weight,
    )
    return out.reshape(rows, d)


def body(sizes, *arrays):
    rows = arrays[0].shape[0]
    heads = arrays[12].shape[0]
    sinks = arrays[14].shape[0]
    n = sizes["sp"]
    fits = (
        sizes["grp"] == 2
        and sizes["tp"] == 2 * CORES
        and n == 2 * CORES
        and heads == CORES
        and sinks == 2 * CORES
        and arrays[6].shape[1] == CORES * HD
        and rows == 2 * WINDOW
    )
    if fits:
        return transposed(n, *arrays)
    return on_device(*arrays)


def solution(mesh):
    return jax.shard_map(
        functools.partial(body, dict(mesh.shape)),
        mesh=mesh,
        in_specs=(
            P(("grp", "sp"), None),
            P(),
            P("sp", "tp"),
            P("sp", "tp"),
            P("sp", "tp"),
            P("sp", "tp"),
            P("sp", "tp"),
            P("sp", "tp"),
            P(),
            P(),
            P(),
            P(),
            P("tp"),
            P(),
            P("tp"),
            P("tp", None),
            P("tp", None),
        ),
        out_specs=P(("grp", "sp"), None),
        check_vma=False,
    )
```

```python
import functools

import jax
import jax.numpy as jnp
from jax import lax
from jax.experimental import pallas as pl
from jax.experimental.pallas import tpu as pltpu
from jax.sharding import PartitionSpec as P

HD = 64
WINDOW = 128


def shifted(value, axis, steps):
    count = lax.axis_size(axis)
    first, last = (max(0, -steps), min(count, count - steps))
    return lax.ppermute(value, axis, [(source, source + steps) for source in range(first, last)])


def rms_norm(values, gain):
    return values * lax.rsqrt(jnp.mean(values * values, axis=-1, keepdims=True) + 1e-06) * gain


def absorb(state, queries, places, keys, values, key_places):
    top, total, summed = state
    scores = jnp.einsum(
        "qhmd,khmd->hmqk", queries, keys, preferred_element_type=jnp.float32
    ) * HD ** (-0.5)
    scores = jnp.where(key_places[None, :] <= places[:, None], scores, -jnp.inf)
    new_top = jnp.maximum(top, jnp.max(scores, axis=-1))
    weights = jnp.exp(scores - new_top[..., None])
    total = jnp.sum(weights, axis=-1)
    summed = jnp.einsum(
        "hmqk,khe->hmqe", weights.astype(jnp.bfloat16), values, preferred_element_type=jnp.float32
    )
    return (new_top, total, summed)


def keep(state, queries, places, keys, values, key_places):
    return state


def diff_attention(queries, places, da_key, da_value, mix_lambda, head_gain):
    rows = queries.shape[0]
    heads = queries.shape[1]
    half = rows // 2
    fresh = (
        jnp.full((heads, 2, half), -1e30, jnp.float32),
        jnp.zeros((heads, 2, half), jnp.float32),
        jnp.zeros((heads, 2, half, 2 * HD), jnp.float32),
    )
    states = (fresh, fresh)
    start = jnp.int32(0)
    keys = lax.all_gather(da_key, "sp", axis=0, tiled=True)
    values = lax.all_gather(da_value, "sp", axis=0, tiled=True)
    key_places = jnp.arange(keys.shape[0], dtype=jnp.int32)
    updated = []
    for section in range(2):
        own_rows = queries[section * half : (section + 1) * half]
        own_places = places[section * half : (section + 1) * half]
        updated.append(
            lax.cond(
                start <= jnp.max(own_places),
                absorb,
                keep,
                states[section],
                own_rows,
                own_places,
                keys,
                values,
                key_places,
            )
        )
    states = tuple(updated)
    blended = []
    for top, total, summed in states:
        maps = summed / total[..., None]
        blended.append(maps[:, 0] - mix_lambda[:, None, None] * maps[:, 1])
    blend = jnp.transpose(jnp.concatenate(blended, axis=1), (1, 0, 2))
    return rms_norm(blend, head_gain).astype(jnp.bfloat16).reshape(rows, heads * 2 * HD)


def window_attention(sw_query, sw_key, sw_value, earlier_key, earlier_value, sink_logit, first):
    rows = sw_query.shape[0]
    sw_heads = sw_query.shape[1]
    kv_heads = sw_key.shape[1]
    groups = sw_heads // kv_heads
    count = rows // WINDOW

    def band(own, earlier_tile):
        tiles = own.reshape(count, WINDOW, kv_heads, HD)
        earlier = jnp.concatenate([earlier_tile[None], tiles[:-1]], axis=0)
        return jnp.concatenate([earlier, tiles], axis=1)

    key_band = band(sw_key, earlier_key)
    value_band = band(sw_value, earlier_value)
    query_tiles = sw_query.reshape(count, WINDOW, kv_heads, groups, HD)
    scores = jnp.einsum(
        "nqhgd,nkhd->nhgqk", query_tiles, key_band, preferred_element_type=jnp.float32
    ) * HD ** (-0.5)
    lag = WINDOW + jnp.arange(WINDOW)[:, None] - jnp.arange(2 * WINDOW)[None, :]
    key_places = (
        first + jnp.arange(count)[:, None] * WINDOW - WINDOW + jnp.arange(2 * WINDOW)[None, :]
    )
    valid = ((lag >= 0) & (lag < WINDOW))[None] & (key_places >= 0)[:, None, :]
    scores = jnp.where(valid[:, None, None], scores, -jnp.inf)
    sink = sink_logit.reshape(kv_heads, groups)[None, :, :, None]
    top = jnp.maximum(jnp.max(scores, axis=-1), sink)
    weights = jnp.exp(scores - top[..., None])
    total = jnp.sum(weights, axis=-1) + jnp.exp(sink - top)
    summed = jnp.einsum(
        "nhgqk,nkhd->nqhgd",
        weights.astype(jnp.bfloat16),
        value_band,
        preferred_element_type=jnp.float32,
    )
    return (
        (summed / jnp.transpose(total, (0, 3, 1, 2))[..., None])
        .astype(jnp.bfloat16)
        .reshape(rows, sw_heads * HD)
    )


def on_device(
    inputs,
    norm_gain,
    da_query_weight,
    da_key_weight,
    da_value_weight,
    sw_query_weight,
    sw_key_weight,
    sw_value_weight,
    da_query_gain,
    da_key_gain,
    sw_query_gain,
    sw_key_gain,
    mix_lambda,
    head_gain,
    sink_logit,
    da_out_weight,
    sw_out_weight,
):
    rows = inputs.shape[0]
    normed = rms_norm(inputs.astype(jnp.float32), norm_gain).astype(jnp.bfloat16)
    pieces = (
        lax.all_gather(da_query_weight, "sp", axis=0, tiled=True),
        lax.all_gather(da_key_weight, "sp", axis=0, tiled=True),
        lax.all_gather(da_value_weight, "sp", axis=0, tiled=True),
        lax.all_gather(sw_query_weight, "sp", axis=0, tiled=True),
        lax.all_gather(sw_key_weight, "sp", axis=0, tiled=True),
        lax.all_gather(sw_value_weight, "sp", axis=0, tiled=True),
    )
    projected = tuple(
        (jnp.dot(normed, piece, preferred_element_type=jnp.float32) for piece in pieces)
    )
    da_heads = da_query_weight.shape[1] // (2 * HD)
    sw_heads = sw_query_weight.shape[1] // HD
    kv_heads = sw_key_weight.shape[1] // HD
    da_query = rms_norm(projected[0].reshape(rows, da_heads, 2, HD), da_query_gain).astype(
        jnp.bfloat16
    )
    da_key = rms_norm(projected[1].reshape(rows, da_heads, 2, HD), da_key_gain).astype(jnp.bfloat16)
    da_value = projected[2].astype(jnp.bfloat16).reshape(rows, da_heads, 2 * HD)
    sw_query = rms_norm(projected[3].reshape(rows, sw_heads, HD), sw_query_gain).astype(
        jnp.bfloat16
    )
    sw_key = rms_norm(projected[4].reshape(rows, kv_heads, HD), sw_key_gain).astype(jnp.bfloat16)
    sw_value = projected[5].astype(jnp.bfloat16).reshape(rows, kv_heads, HD)
    place = lax.axis_index("sp")
    first = place * rows
    earlier_key, earlier_value = shifted(
        (sw_key[rows - WINDOW :], sw_value[rows - WINDOW :]), "sp", 1
    )
    sw_rows = window_attention(
        sw_query, sw_key, sw_value, earlier_key, earlier_value, sink_logit, first
    )
    places = first + jnp.arange(rows, dtype=jnp.int32)
    da_rows = diff_attention(da_query, places, da_key, da_value, mix_lambda, head_gain)
    partial_value = jnp.dot(da_rows, da_out_weight, preferred_element_type=jnp.float32) + jnp.dot(
        sw_rows, sw_out_weight, preferred_element_type=jnp.float32
    )
    return lax.psum(partial_value.astype(jnp.bfloat16), "tp")


MESH = pl.DeviceIdType.MESH
F32, BF16 = jnp.float32, jnp.bfloat16
CORES = 2


def dot(a, b):
    return jnp.dot(a, b, preferred_element_type=F32)


def dot_t(a, b):
    return lax.dot_general(a, b, (((1,), (1,)), ((), ())), preferred_element_type=F32)


def pair_norm(values, gain):
    lane = lax.broadcasted_iota(jnp.int32, values.shape, 1)
    squares = values * values
    low = jnp.sum(jnp.where(lane < HD, squares, 0.0), axis=-1, keepdims=True)
    high = jnp.sum(jnp.where(lane < HD, 0.0, squares), axis=-1, keepdims=True)
    mean = jnp.where(lane < HD, low, high) * (1.0 / HD)
    return values * lax.rsqrt(mean + 1e-06) * gain


PIECES = 4
CUTS = 4
EIGHTHS = (0, 3, 8)
HALVES = len(EIGHTHS) - 1
COLUMNS = 4
SHARES = 4


def kernel(
    n,
    x_hbm,
    da_q_hbm,
    da_k_hbm,
    da_v_hbm,
    sw_q_hbm,
    sw_k_hbm,
    sw_v_hbm,
    norm_gain_hbm,
    da_q_gain_hbm,
    da_k_gain_hbm,
    sw_q_gain_hbm,
    sw_k_gain_hbm,
    head_gain_hbm,
    mix_hbm,
    sink_hbm,
    da_out_hbm,
    sw_out_hbm,
    out_ref,
    x_raw,
    skv_raw,
    norm_gain,
    da_q_gain,
    da_k_gain,
    sw_q_gain,
    sw_k_gain,
    head_gain,
    mix_ref,
    sink_ref,
    wout,
    wp,
    xg,
    wb,
    q_da,
    q_sw,
    kv,
    scal,
    rows_out,
    rows_in,
    sum_out,
    sum_in,
    local_sem,
    x_send,
    x_recv,
    xf_send,
    xf_recv,
    w_send,
    w_recv,
    wy_send,
    wy_recv,
    wc_send,
    wc_recv,
    own_send,
    own_recv,
    kv_send,
    kv_recv,
    sc_send,
    sc_recv,
    wo_send,
    wo_recv,
    r_send,
    r_recv,
    s_send,
    s_recv,
    o_send,
    o_recv,
):
    y = lax.axis_index("grp")
    z = lax.axis_index("sp")
    t = lax.axis_index("tp")
    x = t // CORES
    c = t % CORES
    peer = {"tp": x * CORES + 1 - c}
    across = {"tp": (1 - x) * CORES + c}
    beside = {"grp": 1 - y}
    wide = 2 * HD

    def at(zz, cc):
        return {"sp": zz, "tp": x * CORES + cc}

    def remote(src, dst, send, recv, device):
        return pltpu.make_async_remote_copy(
            src_ref=src,
            dst_ref=dst,
            send_sem=send,
            recv_sem=recv,
            device_id=device,
            device_id_type=MESH,
        )

    def go(copy, when=None):
        if when is None:
            copy.start()
        else:
            pl.when(when)(copy.start)

    barrier = pltpu.get_barrier_semaphore()

    def greet(device):
        pl.semaphore_signal(barrier, inc=1, device_id=device, device_id_type=MESH)

    for k in range(n - 1, 0, -1):
        for cc in range(CORES):
            greet(at(lax.rem(z + k, n), cc))
    greet(across)
    greet(beside)
    greet(peer)

    load_x = pltpu.make_async_copy(x_hbm.at[c], x_raw, local_sem.at[0])
    load_x.start()
    smalls = []
    for i, (source, target) in enumerate(
        (
            (norm_gain_hbm, norm_gain),
            (da_q_gain_hbm, da_q_gain),
            (da_k_gain_hbm, da_k_gain),
            (sw_q_gain_hbm, sw_q_gain),
            (sw_k_gain_hbm, sw_k_gain),
            (head_gain_hbm, head_gain),
            (mix_hbm, mix_ref),
            (sink_hbm, sink_ref),
        )
    ):
        smalls.append(pltpu.make_async_copy(source, target, local_sem.at[1 + i]))
        smalls[-1].start()
    for j, source in enumerate((sw_k_hbm, sw_v_hbm)):
        pltpu.make_async_copy(source, skv_raw.at[j], local_sem.at[9]).start()
    for par in range(CORES):
        for j, source in enumerate((da_q_hbm, da_k_hbm, da_v_hbm, sw_q_hbm)):
            pltpu.make_async_copy(
                source.at[:, :, :, :, pl.ds(par * wide, wide)],
                wp.at[par, :, :, :, :, pl.ds(j * wide, wide)],
                local_sem.at[10],
            ).start()
    for j, source in enumerate((da_out_hbm, sw_out_hbm)):
        pltpu.make_async_copy(source, wout.at[j, c], local_sem.at[11]).start()

    smalls[0].wait()
    load_x.wait()
    for h in range(2):
        for p in range(PIECES):
            values = rms_norm(x_raw[h, p].astype(F32), norm_gain[...])
            xg[z, h, p] = values.astype(BF16)
    pltpu.make_async_copy(skv_raw, skv_raw, local_sem.at[9]).wait()
    for par in range(CORES):
        cols = slice(par * HD, (par + 1) * HD)
        wp[par, :, :, :, :, 4 * wide : 5 * wide] = jnp.concatenate(
            [skv_raw[0, ..., cols], skv_raw[1, ..., cols]], axis=-1
        )
    for load in smalls[1:]:
        load.wait()
    for par in range(CORES):
        scal[c, par, 0:1, :] = jnp.broadcast_to(mix_ref[:, par : par + 1], (1, wide))
        for g in range(2):
            sink = sink_ref[:, 2 * par + g : 2 * par + g + 1]
            scal[c, par, 1 + g : 2 + g, :] = jnp.broadcast_to(sink, (1, wide))
    packed = wp.at[:, :, :, :, :, pl.ds(0, 4 * wide)]
    pltpu.make_async_copy(packed, packed, local_sem.at[10]).wait()
    pl.semaphore_wait(barrier, 3 + (n - 1) * CORES)

    def way(d):
        return 1 - 2 * d

    def cross(zs, p):
        piece = xg.at[zs, x, p]
        return remote(piece, piece, xf_send, xf_recv.at[zs], across)

    owner = c == z // CORES

    def hop(zz, d, k, p):
        source, target = zz - k * way(d), zz + way(d)
        if 0 <= target < n:
            piece = xg.at[source, x, p]
            remote(piece, piece, x_send.at[d], x_recv.at[(source - target - 1) % n, p], {"sp": target}).start()

    def weight_beside(zs, yy, s):
        piece = wb.at[zs, yy, c, s]
        return remote(piece, piece, wy_send, wy_recv.at[(zs - z - 1 + n) % n, s], beside)

    def weight_core(zs, yy, s):
        piece = wb.at[zs, yy, c, s]
        return remote(piece, piece, wc_send, wc_recv, peer)

    def event_x(zz, d, k, p):
        zs = zz - k * way(d)
        piece = xg.at[zs, x, p]
        remote(piece, piece, x_send.at[d], x_recv.at[(zs - zz - 1) % n, p], across).wait_recv()
        if k < n - 1:
            hop(zz, d, k, p)
        cross(zs, p).start()

    def event_w(zs, s):
        piece = wb.at[zs, y, c, s]
        remote(piece, piece, w_send, w_recv.at[(zs - z - 1 + n) % n, s], peer).wait_recv()
        weight_beside(zs, y, s).start()
        weight_core(zs, y, s).start()

    def event_y(zs, s):
        weight_beside(zs, 1 - y, s).wait_recv()
        weight_core(zs, 1 - y, s).start()

    def send_weight(zz, zt, s):
        for cd in range(CORES):
            remote(
                wp.at[zt % CORES, y, cd, s],
                wb.at[zz, y, cd, s],
                w_send,
                w_recv.at[(zz - zt - 1) % n, s],
                at(zt, cd),
            ).start()

    def run(script):
        for zz in range(n):
            for cc in range(CORES):

                @pl.when((z == zz) & (c == cc))
                def _(zz=zz, cc=cc):
                    script(zz, cc)

    tile = xg.shape[1] * xg.shape[2] * xg.shape[3]
    depth = wb.shape[1] * wb.shape[2] * wb.shape[3] * wb.shape[4]
    width = wb.shape[5]

    def lanes(shape):
        return lax.broadcasted_iota(jnp.int32, shape, len(shape) - 1)

    low = lanes((tile, wide)) < HD

    def twice(ref):
        return jnp.concatenate([ref[...], ref[...]], axis=-1)

    normed = pair_norm

    def arrive(b):
        @pl.when(b != z)
        def _():
            block = xg.at[b, 1 - x]
            remote(block, block, xf_send, xf_recv.at[b], across).wait_recv()

    def project(b):
        block = xg[b].reshape(tile, xg.shape[4])
        acc = dot(block[:, 0:depth], wb[0].reshape(depth, width))
        for j in range(1, n):
            acc += dot(block[:, j * depth : (j + 1) * depth], wb[j].reshape(depth, width))
        scale = HD ** (-0.5)

        def heads(values, gain):
            result = normed(values, gain).astype(BF16).astype(F32) * scale
            low_half = jnp.where(low, result, 0.0).astype(BF16)
            high_half = jnp.where(low, 0.0, result).astype(BF16)
            return low_half, high_half

        key = normed(acc[:, wide : 2 * wide], twice(da_k_gain))
        kv[c, b, :, 0:wide] = key.astype(BF16)
        kv[c, b, :, wide : 2 * wide] = acc[:, 2 * wide : 3 * wide].astype(BF16)
        pair = acc[:, 4 * wide : 5 * wide]
        pair = jnp.where(low, normed(pair, twice(sw_k_gain)), pair).astype(BF16)
        row = lax.broadcasted_iota(jnp.int32, (wide, 2 * wide), 0)
        column = lanes((wide, 2 * wide))
        source = column % HD + jnp.where(column < wide, 0, HD)
        doubler = jnp.where(row == source, 1.0, 0.0).astype(BF16)
        kv[c, b, :, 2 * wide : 4 * wide] = dot(pair, doubler).astype(BF16)
        swap(b, c).start()
        low_half, high_half = heads(acc[:, 0:wide], twice(da_q_gain))
        q_da[b, 0] = low_half
        q_da[b, 1] = high_half
        low_half, high_half = heads(acc[:, 3 * wide : 4 * wide], twice(sw_q_gain))
        q_sw[b, 0] = low_half
        q_sw[b, 1] = high_half

    def swap(b, core):
        block = kv.at[core, b]
        return remote(block, block, kv_send, kv_recv.at[b], peer)

    def mine():
        return scal[z // CORES, z % CORES]

    bounds = [tile * e // 8 for e in EIGHTHS]

    def rows_of(half):
        return bounds[half], bounds[half + 1] - bounds[half]

    def windows(items, start, count):
        rows = slice(start, start + count)
        size = 2 * count
        row = lax.broadcasted_iota(jnp.int32, (size, tile), 0)
        head = row[:, 0:1] < count
        row = jnp.where(row < count, row, row - count) + start
        column = lanes((size, tile))
        causal = column <= row
        own_scal = mine()
        sink = jnp.where(head, own_scal[1:2, 0:1], own_scal[2:3, 0:1])
        pairs = [
            (
                kv[c, i, :, 2 * wide : 4 * wide],
                kv[1 - c, jnp.maximum(i - 1 + c, 0), :, 2 * wide : 4 * wide],
            )
            for i in items
        ]
        scores = []
        for i, (near, far) in zip(items, pairs):
            q = q_sw[i, :, rows, :].reshape(size, wide)
            far_ok = (column > row) & (2 * i + c > 0)
            scores.append(
                (
                    jnp.where(causal, dot_t(q, near[:, 0:wide]), -jnp.inf),
                    jnp.where(far_ok, dot_t(q, far[:, 0:wide]), -jnp.inf),
                )
            )
        tops = [
            jnp.maximum(jnp.max(jnp.maximum(*two), axis=-1, keepdims=True), sink) for two in scores
        ]
        weights_of = [[jnp.exp(one - top) for one in two] for two, top in zip(scores, tops)]
        totals = [
            jnp.sum(two[0] + two[1], axis=-1, keepdims=True) + jnp.exp(sink - top)
            for two, top in zip(weights_of, tops)
        ]
        low_part = lanes((count, wide)) < HD
        for i, (near, far), two, total in zip(items, pairs, weights_of, totals):
            two = [one.astype(BF16) for one in two]
            summed = dot(two[0], near[:, wide : 2 * wide]) + dot(two[1], far[:, wide : 2 * wide])
            result = summed / total
            rows_out[i, 1, rows, :] = jnp.where(low_part, result[0:count], result[count:size]).astype(BF16)

    def spread(i, half):
        start, part = rows_of(half)
        rows = slice(start, start + part)
        size = 2 * part
        q = q_da[i, :, rows, :].reshape(size, wide)
        row = lax.broadcasted_iota(jnp.int32, (size, tile), 0)
        row = jnp.where(row < part, row, row - part) + start
        column = lanes((size, tile))
        scores = []
        top = None
        for h in range(2):
            keys = kv[h, 0 : i + 1, :, 0:wide].reshape((i + 1) * tile, wide)
            s = dot_t(q, keys)
            tiles = [s[:, j * tile : (j + 1) * tile] for j in range(i + 1)]
            tiles[i] = jnp.where(column + (h - c) * tile <= row, tiles[i], -jnp.inf)
            scores.append(tiles)
            for one in tiles:
                top = one if top is None else jnp.maximum(top, one)
        top = jnp.max(top, axis=-1, keepdims=True)
        total = None
        summed = None
        for h in range(2):
            weights = [jnp.exp(one - top) for one in scores[h]]
            for one in weights:
                total = one if total is None else total + one
            values = kv[h, 0 : i + 1, :, wide : 2 * wide].reshape((i + 1) * tile, wide)
            flat = jnp.concatenate([one.astype(BF16) for one in weights], axis=-1)
            step = dot(flat, values)
            summed = step if summed is None else summed + step
        total = jnp.sum(total, axis=-1, keepdims=True)
        maps = summed / total
        blend = maps[0:part] - mine()[0:1, :] * maps[part:size]
        return rms_norm(blend, head_gain[...]).astype(BF16)

    def send_rows(i, j, half):
        rows = pl.ds(*rows_of(half))
        go(
            remote(
                rows_out.at[i, j, rows],
                rows_in.at[j, z, rows],
                r_send,
                r_recv.at[j, half],
                {"sp": i},
            ),
            z != i,
        )

        @pl.when(z == i)
        def _():
            rows = slice(bounds[half], bounds[half + 1])
            rows_in[j, i, rows, :] = rows_out[i, j, rows, :]

    def await_rows(j, half):
        block = rows_in.at[j, 0 : n - 1, pl.ds(*rows_of(half))]
        remote(block, block, r_send, r_recv.at[j, half], peer).wait_recv()

    def opening(zz, cc):
        targets = [zt for zt in (CORES * cc, CORES * cc + 1) if zt != zz]
        targets.sort(key=lambda zt: -abs(zt - zz))
        for s in range(CUTS):
            for zt in targets:
                send_weight(zz, zt, s)
        for p in range(PIECES):
            for d in range(2):
                hop(zz, d, 0, p)

    def reach(zz, d):
        return zz if d == 0 else n - 1 - zz

    def steps(ends, mids):
        def script(zz, cc):
            for kind, k, p in ends if zz in (0, n - 1) else mids:
                if kind == "W":
                    for far in range(1, n):
                        for d in range(2):
                            if far <= reach(zz, d):
                                event_w(zz - far * way(d), p)
                elif kind == "Y":
                    for far in range(1, n):
                        for d in range(2):
                            if far <= reach(zz, d):
                                event_y(zz - far * way(d), p)
                else:
                    d = cc if kind == "E" else 1 - cc
                    if k <= reach(zz, d):
                        event_x(zz, d, k, p)

        return script

    blocks = (
        z,
        z + 1 - 2 * (z % 2),
        jnp.where(z < 2, 2, 1),
        jnp.where(z < 2, 3, 0),
    )

    own_w = remote(wp.at[z % CORES], wb.at[z], own_send, own_recv, peer)
    own_local = pltpu.make_async_copy(wp.at[z % CORES], wb.at[z], local_sem.at[12])
    sc = remote(scal.at[c], scal.at[c], sc_send, sc_recv, peer)

    def share(j, part):
        rows = wout.shape[2] // SHARES
        block = wout.at[j, c, pl.ds(part * rows, rows)]
        return remote(block, block, wo_send, wo_recv, peer)

    def share_all():
        pltpu.make_async_copy(wout.at[:, c], wout.at[:, c], local_sem.at[11]).wait()
        for j in range(2):
            for part in range(SHARES):
                share(j, part).start()


    run(opening)
    go(own_w, owner)
    pl.when(owner)(own_local.start)
    go(sc)

    run(steps((("E", 1, 0), ("W", 0, 0), ("E", 1, 1), ("W", 0, 1), ("E", 1, 2), ("E", 2, 0), ("E", 1, 3), ("E", 2, 1), ("W", 0, 2), ("L", 1, 0), ("E", 2, 2), ("L", 1, 1), ("W", 0, 3), ("L", 1, 2), ("Y", 0, 0), ("E", 2, 3), ("L", 1, 3), ("Y", 0, 1), ("E", 3, 0), ("E", 3, 1), ("Y", 0, 2), ("E", 3, 2), ("L", 2, 0), ("E", 3, 3), ("L", 2, 1), ("L", 2, 2), ("L", 2, 3), ("Y", 0, 3)), (("E", 1, 0), ("W", 0, 0), ("E", 1, 1), ("W", 0, 1), ("E", 1, 2), ("E", 1, 3), ("W", 0, 2), ("E", 2, 0), ("E", 2, 1), ("W", 0, 3), ("L", 1, 0), ("E", 2, 2), ("L", 1, 1), ("E", 2, 3), ("L", 1, 2), ("Y", 0, 0), ("L", 1, 3), ("Y", 0, 1), ("L", 2, 0), ("Y", 0, 2), ("L", 2, 1), ("L", 2, 2), ("L", 2, 3), ("Y", 0, 3))))
    pl.when(owner)(own_local.wait)
    pl.when(jnp.logical_not(owner))(own_w.wait_recv)
    theirs = wb.at[0 : n - 1, :, 1 - c]
    remote(theirs, theirs, wc_send, wc_recv, peer).wait_recv()
    run(steps((("L", 3, 0),), ()))
    project(blocks[0])
    run(steps((("L", 3, 1),), ()))
    arrive(blocks[1])
    project(blocks[1])
    run(steps((("L", 3, 2), ("L", 3, 3)), ()))
    arrive(blocks[2])
    project(blocks[2])
    remote(scal.at[1 - c], scal.at[1 - c], sc_send, sc_recv, peer).wait_recv()
    for b in blocks[:3]:
        swap(b, 1 - c).wait_recv()
    windows((jnp.where(z < 2, 1, 3), 2), 0, tile)
    arrive(blocks[3])
    project(blocks[3])
    share_all()
    swap(blocks[3], 1 - c).wait_recv()
    for half in range(HALVES):
        rows = slice(bounds[half], bounds[half + 1])
        windows((jnp.where(z < 2, 0, 1), jnp.where(z < 2, 3, 0)), *rows_of(half))
        for i in (3, 0, 2, 1):
            send_rows(i, 1, half)
        for i in (3, 0):
            rows_out[i, 0, rows, :] = spread(i, half)
        for i in (3, 0):
            send_rows(i, 0, half)
        for i in (2, 1):
            rows_out[i, 0, rows, :] = spread(i, half)
        for i in (2, 1):
            send_rows(i, 0, half)

    share_in = wout.at[:, 1 - c]
    remote(share_in, share_in, wo_send, wo_recv, peer).wait_recv()
    columns = out_ref.shape[2] // COLUMNS

    def span(half, q):
        return pl.ds(*rows_of(half)), pl.ds(q * columns, columns)

    def summing(half, q):
        rows, cols = span(half, q)
        return remote(
            sum_out.at[rows, cols],
            sum_in.at[rows, cols],
            s_send,
            s_recv.at[half, q],
            across,
        )

    def finish(half, q):
        rows, cols = span(half, q)
        summing(half, q).wait_recv()
        out_ref[c, rows, cols] = (sum_out[rows, cols].astype(F32) + sum_in[rows, cols].astype(F32)).astype(BF16)
        block = out_ref.at[c, rows, cols]
        go(remote(block, block, o_send, o_recv, peer))

    for half in range(HALVES):
        rows = slice(bounds[half], bounds[half + 1])
        await_rows(1, half)
        await_rows(0, half)
        for q in range(COLUMNS):
            cols = slice(q * columns, (q + 1) * columns)
            acc = None
            for j in range(2):
                values = jnp.concatenate([rows_in[j, zs, rows, :] for zs in range(n)], axis=-1)
                step = dot(values, wout[j, :, :, cols].reshape(2 * wout.shape[2], columns))
                acc = step if acc is None else acc + step
            sum_out[rows, cols] = acc.astype(BF16)
            go(summing(half, q))
    for half in range(HALVES):
        for q in range(COLUMNS):
            finish(half, q)
    block = out_ref.at[1 - c]
    remote(block, block, o_send, o_recv, peer).wait_recv()

    def drained(ref, sem):
        remote(ref, ref, sem, o_recv, peer).wait_send()

    for zz in range(n):

        @pl.when(z == zz)
        def _(zz=zz):
            if zz + 1 < n:
                drained(xg.at[0 : zz + 1, x], x_send.at[0])
            if zz >= 1:
                drained(xg.at[0 : n - zz, x], x_send.at[1])

    drained(xg.at[0 : n - 1, x], xf_send)
    pl.when(owner)(lambda: drained(wp.at[0, y], w_send))
    pl.when(jnp.logical_not(owner))(lambda: drained(wp.at[:, y], w_send))
    pl.when(owner)(lambda: drained(wp.at[0], own_send))
    drained(wb.at[0 : n - 1, y, c], wy_send)
    drained(wb.at[0 : n - 1, :, c], wc_send)
    drained(scal.at[c], sc_send)
    drained(wout.at[:, c], wo_send)
    drained(kv.at[c], kv_send)
    drained(rows_out.at[0 : n - 1], r_send)
    drained(sum_out, s_send)
    drained(out_ref.at[c], o_send)


def transposed(n, *arrays):
    (
        inputs,
        norm_gain,
        da_query_weight,
        da_key_weight,
        da_value_weight,
        sw_query_weight,
        sw_key_weight,
        sw_value_weight,
        da_query_gain,
        da_key_gain,
        sw_query_gain,
        sw_key_gain,
        mix_lambda,
        head_gain,
        sink_logit,
        da_out_weight,
        sw_out_weight,
    ) = arrays
    rows, d = inputs.shape
    depth = da_query_weight.shape[0]
    wide = 2 * HD
    width = 5 * wide
    cut_rows = depth // 4 // CUTS
    tile = rows // 2
    part = tile // 2 // PIECES
    group = da_out_weight.shape[0]

    def cut(weight):
        return weight.reshape(2, CORES, CUTS, cut_rows, weight.shape[1])

    def line(vector):
        return vector.reshape(1, -1)

    DMA = pltpu.SemaphoreType.DMA
    any_space = pl.BlockSpec(memory_space=pl.ANY)
    out = pl.pallas_call(
        functools.partial(kernel, n),
        out_shape=pltpu.VMEM((2, tile, d), BF16),
        in_specs=[any_space] * 17,
        out_specs=pl.BlockSpec(memory_space=pltpu.VMEM),
        scratch_shapes=[
            pltpu.VMEM((2, PIECES, part, d), BF16),
            pltpu.VMEM((2, 2, CORES, CUTS, cut_rows, wide), BF16),
            pltpu.VMEM((1, d), F32),
            pltpu.VMEM((1, HD), F32),
            pltpu.VMEM((1, HD), F32),
            pltpu.VMEM((1, HD), F32),
            pltpu.VMEM((1, HD), F32),
            pltpu.VMEM((1, wide), F32),
            pltpu.VMEM((1, mix_lambda.shape[0]), F32),
            pltpu.VMEM((1, sink_logit.shape[0]), F32),
            pltpu.VMEM((2, CORES, group, d), BF16),
            pltpu.VMEM((CORES, 2, CORES, CUTS, cut_rows, width), BF16),
            pltpu.VMEM((n, 2, PIECES, part, d), BF16),
            pltpu.VMEM((n, 2, CORES, CUTS, cut_rows, width), BF16),
            pltpu.VMEM((n, 2, tile, wide), BF16),
            pltpu.VMEM((n, 2, tile, wide), BF16),
            pltpu.VMEM((CORES, n, tile, 4 * wide), BF16),
            pltpu.VMEM((CORES, CORES, 8, wide), F32),
            pltpu.VMEM((n, 2, tile, wide), BF16),
            pltpu.VMEM((2, n, tile, wide), BF16),
            pltpu.VMEM((tile, d), BF16),
            pltpu.VMEM((tile, d), BF16),
            DMA((13,)),
            DMA((2,)),
            DMA((n - 1, PIECES)),
            DMA,
            DMA((n,)),
            DMA,
            DMA((n - 1, CUTS)),
            DMA,
            DMA((n - 1, CUTS)),
            DMA,
            DMA,
            DMA,
            DMA,
            DMA,
            DMA((n,)),
            DMA,
            DMA,
            DMA,
            DMA,
            DMA,
            DMA((2, HALVES)),
            DMA,
            DMA((HALVES, COLUMNS)),
            DMA,
            DMA,
        ],
        compiler_params=pltpu.CompilerParams(
            collective_id=0, has_side_effects=True, vmem_limit_bytes=60 * 1024 * 1024
        ),
    )(
        inputs.reshape(CORES, 2, PIECES, part, d),
        cut(da_query_weight),
        cut(da_key_weight),
        cut(da_value_weight),
        cut(sw_query_weight),
        cut(sw_key_weight),
        cut(sw_value_weight),
        line(norm_gain),
        line(da_query_gain),
        line(da_key_gain),
        line(sw_query_gain),
        line(sw_key_gain),
        line(head_gain),
        line(mix_lambda),
        line(sink_logit),
        da_out_weight,
        sw_out_weight,
    )
    return out.reshape(rows, d)


def body(sizes, *arrays):
    rows = arrays[0].shape[0]
    heads = arrays[12].shape[0]
    sinks = arrays[14].shape[0]
    n = sizes["sp"]
    fits = (
        sizes["grp"] == 2
        and sizes["tp"] == 2 * CORES
        and n == 2 * CORES
        and heads == CORES
        and sinks == 2 * CORES
        and arrays[6].shape[1] == CORES * HD
        and rows == 2 * WINDOW
    )
    if fits:
        return transposed(n, *arrays)
    return on_device(*arrays)


def solution(mesh):
    return jax.shard_map(
        functools.partial(body, dict(mesh.shape)),
        mesh=mesh,
        in_specs=(
            P(("grp", "sp"), None),
            P(),
            P("sp", "tp"),
            P("sp", "tp"),
            P("sp", "tp"),
            P("sp", "tp"),
            P("sp", "tp"),
            P("sp", "tp"),
            P(),
            P(),
            P(),
            P(),
            P("tp"),
            P(),
            P("tp"),
            P("tp", None),
            P("tp", None),
        ),
        out_specs=P(("grp", "sp"), None),
        check_vma=False,
    )
```
